256 devices in a mesh: sp: 64 (over z, y, core), tp: 4 (over x).
Axes of the slice: x: 4, y: 4, z: 8, core: 2. Of those that a mesh axis runs over, the one named last changes fastest.
Arguments:
- tokens: bfloat16 [49152, 2048], P('sp', 'tp'), may hold values from -12 to 12
- query_weight: bfloat16 [2048, 1024], P('sp', 'tp'), may hold values from -0.176776695 to 0.176776695
- key_projection: bfloat16 [2048, 512], P('sp', 'tp'), may hold values from -0.176776695 to 0.176776695
- value_projection: bfloat16 [2048, 512], P('sp', 'tp'), may hold values from -0.125 to 0.125
- conv_in_weight: bfloat16 [2048, 1024], P('sp', 'tp'), may hold values from -0.125 to 0.125
- conv_gate_out: bfloat16 [2048, 1024], P('sp', 'tp'), may hold values from -0.125 to 0.125
- conv_gate_in: bfloat16 [2048, 1024], P('sp', 'tp'), may hold values from -0.125 to 0.125
- conv_taps: bfloat16 [3, 1024], P(None, 'tp'), may hold values from -3 to 3
- head_sink_logit: float32 [8], P('tp'), may hold values from 3 to 8
- out_attn_weight: bfloat16 [1024, 2048], P('tp', 'sp'), may hold values from -5 to 5
- out_conv_weight: bfloat16 [1024, 2048], P('tp', 'sp'), may hold values from -0.5 to 0.5
- out_gain: float32 [2048], P('tp'), may hold values from 0.1 to 1.9
Outputs:
- mixed: bfloat16 [49152, 2048], P('sp', 'tp')
The draws below stay inside these ranges and needn't reach their ends.
All inputs are finite; a program needn't handle non-finite values.
Results may differ from the reference program's by a relative error of at most 0.014.
Values may be sent and summed in bfloat16 or wider, within the bound.
A program may use at most 64 MiB of HBM per device.

```python
import jax
import jax.numpy as jnp
from jax import lax

MODEL_WIDTH = 2048
HEAD_SIZE = 128
QUERY_HEADS = 8
KEY_VALUE_HEADS = 4
CONV = 1024
WINDOW = 128
GRID = 64
TOKENS = 49152


def draw_tokens(key, part):
    base = jnp.clip(jax.random.normal(jax.random.fold_in(key, 3), (TOKENS, MODEL_WIDTH), jnp.float32), -6.0, 6.0)
    return jnp.clip(base, -12.0, 12.0).astype(jnp.bfloat16)


def query_key_pair(key):
    head_group = QUERY_HEADS // KEY_VALUE_HEADS
    limit_value = 8.0 * MODEL_WIDTH ** (-0.5)
    query_portion = jnp.clip(jax.random.normal(jax.random.fold_in(key, 21), (MODEL_WIDTH, KEY_VALUE_HEADS, head_group, HEAD_SIZE), jnp.float32), -6.0, 6.0)
    key_portion = jnp.clip(jax.random.normal(jax.random.fold_in(key, 22), (MODEL_WIDTH, KEY_VALUE_HEADS, 1, HEAD_SIZE), jnp.float32), -6.0, 6.0)
    query_matrix = jnp.clip(query_portion.reshape(MODEL_WIDTH, QUERY_HEADS * HEAD_SIZE) * MODEL_WIDTH ** (-0.5), -limit_value, limit_value)
    key_projected = jnp.clip(key_portion.reshape(MODEL_WIDTH, KEY_VALUE_HEADS * HEAD_SIZE) * MODEL_WIDTH ** (-0.5), -limit_value, limit_value)
    return (query_matrix, key_projected)


def draw_query_weight(key, part):
    return query_key_pair(key)[0].astype(jnp.bfloat16)


def draw_key_projection(key, part):
    return query_key_pair(key)[1].astype(jnp.bfloat16)


def out_block(key, salt, rows, factor, limit):
    base = jnp.clip(jax.random.normal(jax.random.fold_in(key, salt), (rows, MODEL_WIDTH), jnp.float32), -6.0, 6.0)
    common = 0.7 * jnp.clip(jax.random.normal(jax.random.fold_in(key, salt + 1), (rows, 1), jnp.float32), -6.0, 6.0)
    column = jnp.arange(MODEL_WIDTH, dtype=jnp.int32).astype(jnp.float32) / (MODEL_WIDTH - 1)
    exponent = column - 0.5
    scale = (10.0 ** exponent)[None, :]
    value_rows = (base + common) * scale * factor * rows ** (-0.5)
    return jnp.clip(value_rows, -limit * rows ** (-0.5), limit * rows ** (-0.5)).astype(jnp.bfloat16)


def draw_out_attn_weight(key, part):
    return out_block(key, 41, QUERY_HEADS * HEAD_SIZE, 5.0, 160.0)


def draw_out_conv_weight(key, part):
    return out_block(key, 51, CONV, 0.5, 16.0)


def shard_levels(rng, dims, cuts, smallest, largest):
    def one(dim, parts):
        steps = jax.random.uniform(jax.random.fold_in(jax.random.fold_in(rng, 6), dim), (parts,), jnp.float32, smallest / len(cuts), largest / len(cuts))
        return jnp.repeat(jnp.exp(steps), dims[dim] // parts).reshape((-1,) + (1,) * (len(dims) - dim - 1))

    factor_of = one(*cuts[0])
    for cut in cuts[1:]:
        factor_of = factor_of * one(*cut)
    return factor_of


def scatter_about(stream_key, dims, scale, most, shards=(), kind=jnp.bfloat16):
    array = scale * jax.random.normal(stream_key, dims, jnp.float32)
    if shards:
        array = array * shard_levels(stream_key, dims, shards, -0.22, 0.18)
    return jnp.clip(array, -most, most).astype(kind)


def setup_inputs(seed: int = 0) -> dict:
    key_list = jax.random.split(jax.random.key(seed), 13)
    return {
        "tokens": draw_tokens(jax.random.fold_in(key_list[12], 71), 0),
        "query_weight": draw_query_weight(jax.random.fold_in(key_list[12], 71), 0),
        "key_projection": draw_key_projection(jax.random.fold_in(key_list[12], 71), 0),
        "value_projection": scatter_about(key_list[3], (MODEL_WIDTH, KEY_VALUE_HEADS * HEAD_SIZE), MODEL_WIDTH ** -0.5, 0.125, ((0, 64), (1, 4))),
        "conv_in_weight": scatter_about(key_list[4], (MODEL_WIDTH, CONV), MODEL_WIDTH ** -0.5, 0.125, ((0, 64), (1, 4))),
        "conv_gate_out": scatter_about(key_list[5], (MODEL_WIDTH, CONV), MODEL_WIDTH ** -0.5, 0.125, ((0, 64), (1, 4))),
        "conv_gate_in": scatter_about(key_list[6], (MODEL_WIDTH, CONV), MODEL_WIDTH ** -0.5, 0.125, ((0, 64), (1, 4))),
        "conv_taps": scatter_about(key_list[7], (3, CONV), 0.6, 3.0, ((1, 4),)),
        "head_sink_logit": jnp.clip(3.0 + 5.0 * jax.random.uniform(key_list[8], (QUERY_HEADS,), jnp.float32) ** shard_levels(key_list[8], (QUERY_HEADS,), ((0, 4),), -0.2, 0.2), 3.0, 8.0),
        "out_attn_weight": draw_out_attn_weight(jax.random.fold_in(key_list[12], 71), 0),
        "out_conv_weight": draw_out_conv_weight(jax.random.fold_in(key_list[12], 71), 0),
        "out_gain": jnp.clip(1.0 + 0.18 * jax.random.normal(key_list[11], (MODEL_WIDTH,), jnp.float32), 0.1, 1.9),
    }


NEG_BIG = -1e+30
THETA = 10000.0
EPS = 1e-05

def rope_tables(positions):
    row = (positions // GRID).astype(jnp.float32)
    column = (positions % GRID).astype(jnp.float32)
    half = HEAD_SIZE // 2
    inverse = THETA ** (-jnp.arange(0, half, 2, dtype=jnp.float32) / half)
    angle_row = row[:, None] * inverse
    angle_col = column[:, None] * inverse
    angles = jnp.concatenate([angle_row, angle_row, angle_col, angle_col], -1)
    return (jnp.cos(angles)[:, None, :], jnp.sin(angles)[:, None, :])

def rotate(vectors, cosine, sine):
    first, second, third, fourth = jnp.split(vectors, 4, axis=-1)
    turned = jnp.concatenate([-second, first, -fourth, third], -1)
    return vectors * cosine + turned * sine

def band_head(inputs):
    query_vectors, key_rows, value_rows, sink = inputs
    item_count = query_vectors.shape[0]
    blocks = item_count // WINDOW

    def band(block):
        padded = jnp.pad(block, ((WINDOW, WINDOW), (0, 0))).reshape(blocks + 2, WINDOW, HEAD_SIZE)
        return jnp.concatenate([padded[:-2], padded[1:-1], padded[2:]], axis=1)
    query_blocks = query_vectors.reshape(blocks, WINDOW, -1, HEAD_SIZE).astype(jnp.float32)
    key_band = band(key_rows).astype(jnp.float32)
    value_band = band(value_rows).astype(jnp.float32)
    scores = jnp.einsum('nqgd,nkd->ngqk', query_blocks, key_band) * HEAD_SIZE ** (-0.5)
    block_start = jnp.arange(blocks, dtype=jnp.int32)[:, None] * WINDOW
    query_pos = block_start + jnp.arange(WINDOW, dtype=jnp.int32)[None, :]
    key_pos = block_start - WINDOW + jnp.arange(3 * WINDOW, dtype=jnp.int32)[None, :]
    distance = key_pos[:, None, :] - query_pos[:, :, None]
    valid = (jnp.abs(distance) <= WINDOW) & (key_pos[:, None, :] >= 0) & (key_pos[:, None, :] < item_count)
    scores = jnp.where(valid[:, None], scores, NEG_BIG)
    sink_col = sink.astype(jnp.float32).reshape(1, -1, 1, 1)
    top = jnp.maximum(lax.optimization_barrier(jnp.max(scores, -1, keepdims=True)), sink_col)
    weights = jnp.exp(scores - top)
    denominator = lax.optimization_barrier(jnp.sum(weights, -1, keepdims=True)) + jnp.exp(sink_col - top)
    probs = lax.optimization_barrier((weights / denominator).astype(jnp.bfloat16)).astype(jnp.float32)
    mixed = jnp.einsum('ngqk,nkd->nqgd', probs, value_band)
    return mixed.reshape(item_count, -1, HEAD_SIZE).astype(jnp.bfloat16)

def reference(tokens, query_weight, key_projection, value_projection, conv_in_weight, conv_gate_out, conv_gate_in, conv_taps, head_sink_logit, out_attn_weight, out_conv_weight, out_gain):
    item_count = tokens.shape[0]
    head_group = QUERY_HEADS // KEY_VALUE_HEADS
    positions = jnp.arange(item_count, dtype=jnp.int32)
    cosine, sine = rope_tables(positions)
    query_raw = jnp.dot(tokens, query_weight, preferred_element_type=jnp.float32).reshape(item_count, QUERY_HEADS, HEAD_SIZE)
    query_vectors = rotate(query_raw, cosine, sine).astype(jnp.bfloat16)
    key_unrotated = jnp.dot(tokens, key_projection, preferred_element_type=jnp.float32).reshape(item_count, KEY_VALUE_HEADS, HEAD_SIZE)
    key_rows = rotate(key_unrotated, cosine, sine).astype(jnp.bfloat16)
    value_rows = jnp.dot(tokens, value_projection, preferred_element_type=jnp.float32).astype(jnp.bfloat16)
    value_rows = value_rows.reshape(item_count, KEY_VALUE_HEADS, HEAD_SIZE)
    head_major = (jnp.transpose(query_vectors.reshape(item_count, KEY_VALUE_HEADS, head_group, HEAD_SIZE), (1, 0, 2, 3)), jnp.transpose(key_rows, (1, 0, 2)), jnp.transpose(value_rows, (1, 0, 2)), head_sink_logit.reshape(KEY_VALUE_HEADS, head_group))
    mixed_heads = lax.map(band_head, head_major)
    attention_out = jnp.transpose(mixed_heads, (1, 0, 2, 3)).reshape(item_count, QUERY_HEADS * HEAD_SIZE)
    conv_input = jnp.dot(tokens, conv_in_weight, preferred_element_type=jnp.float32)
    gate_after = jnp.dot(tokens, conv_gate_out, preferred_element_type=jnp.float32)
    gate_before = jnp.dot(tokens, conv_gate_in, preferred_element_type=jnp.float32)
    sectioned = (gate_before * conv_input).astype(jnp.bfloat16)
    padded = jnp.pad(sectioned, ((1, 1), (0, 0))).astype(jnp.float32)
    taps = conv_taps.astype(jnp.float32)
    conv_mix = padded[:-2] * taps[0] + padded[1:-1] * taps[1] + padded[2:] * taps[2]
    conv_out = (gate_after * conv_mix).astype(jnp.bfloat16)
    summed = jnp.dot(attention_out, out_attn_weight, preferred_element_type=jnp.float32) + jnp.dot(conv_out, out_conv_weight, preferred_element_type=jnp.float32)
    mean = lax.optimization_barrier(jnp.mean(summed, -1, keepdims=True))
    spread = lax.optimization_barrier(jnp.mean(jnp.square(summed - mean), -1, keepdims=True))
    return ((summed - mean) * lax.rsqrt(spread + EPS) * out_gain).astype(jnp.bfloat16)
```

```python
import functools

import jax
import jax.numpy as jnp
import numpy as np
from jax import lax
from jax.experimental import pallas as pl
from jax.experimental.pallas import tpu as pltpu
from jax.sharding import PartitionSpec as P

MESH = pl.DeviceIdType.MESH
F32 = jnp.float32
BF16 = jnp.bfloat16

HEAD = 128
WINDOW = 128
GRID = 64
NEG_BIG = -1e30
THETA = 10000.0
EPS = 1e-05

NZ, NY, NX, NSP = 8, 4, 4, 64
ROWS = 768
WIDTH = 2048
QUARTER = 512
CA = 768
CB = 1024
ORDER = (0, 5, 1, 2, 3, 4)
CHUNKS = ((0, 128, 0), (128, 128, 640), (256, 256, 128), (512, 256, 384))


def nt_dot(a, b):
    return lax.dot_general(a, b, (((1,), (1,)), ((), ())), preferred_element_type=F32)


def kernel(
    tok, qw, kw, vw, cin, cgo, cgi, taps_in, sink, owa, owc, gain_in, freq_in, out,
    T, WA, WB, KV, Q, SEC, GA, MIX, ES, ER, COS, SIN, S2, PT, PB, PX, S1, R2, R1, ST, OUT,
    owa_v, owc_v, taps_v, gain_v, freq_v,
    lsem, ssem, wrec, srec, irec, xrec, hrec, r2rec, r1rec, strec, osem,
):
    s = lax.axis_index("sp")
    x = lax.axis_index("tp")
    core = s % 2
    chip = s // 2
    y = chip % NY
    z = chip // NY

    def at(zz, yy, cc):
        return ((zz % NZ) * NY + yy % NY) * 2 + cc

    sib = (at(z, y, 1 - core), x)
    yp, ym, y2 = [(at(z, y + d, core), x) for d in (1, 3, 2)]
    zp, zm = [(at(z + d, y, core), x) for d in (1, NZ - 1)]
    xp, xm, x2 = [(s, (x + d) % NX) for d in (1, 3, 2)]
    sp, sm = [((s + d) % NSP, x) for d in (1, NSP - 1)]

    loads = []

    def load(src, dst):
        cp = pltpu.make_async_copy(src, dst, lsem.at[len(loads)])
        cp.start()
        loads.append(cp)
        return cp

    own_cols = pl.ds(pl.multiple_of(x * QUARTER, QUARTER), QUARTER)
    own_rows = pl.ds(pl.multiple_of(core * 32, 32), 32)
    l_out = [load(owa, owa_v), load(owc, owc_v)]
    l_w = [
        load(qw, WA.at[z, y, own_rows, pl.ds(0, 256)]),
        load(kw, WA.at[z, y, own_rows, pl.ds(256, 128)]),
        load(vw, WA.at[z, y, own_rows, pl.ds(384, 128)]),
        load(cin, WB.at[z, y, own_rows, pl.ds(0, 256)]),
        load(cgo, WB.at[z, y, own_rows, pl.ds(256, 256)]),
        load(cgi, WB.at[z, y, own_rows, pl.ds(512, 256)]),
    ]
    l_t = [
        load(tok.at[pl.ds(src, n), :], T.at[pl.ds(dst, n), own_cols])
        for dst, n, src in CHUNKS
    ]
    l_small = [load(taps_in, taps_v), load(gain_in, gain_v), load(freq_in, freq_v)]

    barrier = pltpu.get_barrier_semaphore()
    peers = (sib, yp, ym, y2, zp, zm, xp, xm, x2, sp, sm)
    for peer in peers:
        pl.semaphore_signal(barrier, inc=1, device_id=peer, device_id_type=MESH)

    for cp in l_out:
        cp.wait()
    eye = jnp.where(
        lax.broadcasted_iota(jnp.int32, (32, 32), 0)
        == lax.broadcasted_iota(jnp.int32, (32, 32), 1),
        1.0,
        0.0,
    ).astype(BF16)
    WA[z, y, own_rows, 512:768] = nt_dot(eye, owa_v[...]).astype(BF16)
    WB[z, y, own_rows, 768:1024] = nt_dot(eye, owc_v[...]).astype(BF16)

    for cp in l_w:
        cp.wait()
    pl.semaphore_wait(barrier, len(peers))

    sent = []

    def copy(src, dst, rsem, peer, k=0):
        return pltpu.make_async_remote_copy(
            src_ref=src, dst_ref=dst, send_sem=ssem.at[k], recv_sem=rsem,
            device_id=peer, device_id_type=MESH,
        )

    def send(src, dst, rsem, peer, like=None):
        cp = copy(src, dst, rsem, peer, len(sent))
        cp.start()
        sent.append(cp if like is None else like)

    def arrived(ref, rsem):
        copy(ref, ref, rsem, xp).wait_recv()

    ownA = WA.at[z, y, own_rows]
    ownB = WB.at[z, y, own_rows]
    sib_rows = pl.ds(pl.multiple_of((1 - core) * 32, 32), 32)
    sibA = WA.at[z, y, sib_rows]
    sibB = WB.at[z, y, sib_rows]
    send(ownA, ownA, irec.at[0], sib)
    send(ownB, ownB, irec.at[1], sib)

    def cols(d):
        return pl.ds(pl.multiple_of(((x + d) % NX) * QUARTER, QUARTER), QUARTER)

    for i, (dst, n, _) in enumerate(CHUNKS):
        l_t[i].wait()
        blk = T.at[pl.ds(dst, n), own_cols]
        send(blk, blk, xrec.at[i], xp)
        send(blk, blk, xrec.at[4 + i], xm)

    RELAY = (
        ((0, 0, 128, 1),),
        ((1, 128, 128, -1),),
        ((2, 256, 128, 1), (2, 384, 128, -1)),
        ((3, 512, 128, 1), (3, 640, 128, -1)),
    )

    def t_chunk(i, d):
        dst, n, _ = CHUNKS[i]
        return T.at[pl.ds(dst, n), cols(d)]

    def x_relay(i):
        for _, r0, n, direction in RELAY[i]:
            if direction == 1:
                arrived(t_chunk(i, 3), xrec.at[i])
                blk = T.at[pl.ds(r0, n), cols(3)]
                send(blk, blk, xrec.at[8 + r0 // 128], xp, "t")
            else:
                arrived(t_chunk(i, 1), xrec.at[4 + i])
                blk = T.at[pl.ds(r0, n), cols(1)]
                send(blk, blk, xrec.at[8 + r0 // 128], xm, "t")

    def x_rest(i):
        if i == 0:
            arrived(t_chunk(0, 1), xrec.at[4])
            arrived(T.at[pl.ds(0, 128), cols(2)], xrec.at[8])
        elif i == 1:
            arrived(t_chunk(1, 3), xrec.at[1])
            arrived(T.at[pl.ds(128, 128), cols(2)], xrec.at[9])
        else:
            r0 = CHUNKS[i][0]
            arrived(T.at[pl.ds(r0, 128), cols(2)], xrec.at[8 + r0 // 128])
            arrived(T.at[pl.ds(r0 + 128, 128), cols(2)], xrec.at[9 + r0 // 128])

    def rel(dz, dy):
        return (dz % NZ) * NY + dy % NY

    def run_a():
        def piece(dz, dy):
            return WA.at[(z + dz) % NZ, (y + dy) % NY]

        def fwd(dz, dy, peer, ddz, ddy):
            p = piece(dz, dy)
            send(p, p, wrec.at[rel(dz + ddz, dy + ddy)], peer, "a")

        def to_sib(dz, dy):
            p = piece(dz, dy)
            send(p, p, srec.at[rel(dz, dy)], sib, "a")

        def got(dz, dy):
            arrived(piece(dz, dy), wrec.at[rel(dz, dy)])

        arrived(sibA, irec.at[0])
        fwd(0, 0, zp, -1, 0)
        fwd(0, 0, zm, 1, 0)
        fwd(0, 0, yp, 0, -1)
        fwd(0, 0, ym, 0, 1)
        fwd(0, 0, y2, 0, 2)
        for dy in (1, 3, 2):
            got(0, dy)
            fwd(0, dy, zp, -1, 0)
            fwd(0, dy, zm, 1, 0)
            to_sib(0, dy)
        for k in (1, 2, 3):
            for n, dy in enumerate((0, 1, 3, 2)):
                got(-k, dy)
                if k < 3 or n % 2 == 0:
                    fwd(-k, dy, zp, -1, 0)
                to_sib(-k, dy)
                got(k, dy)
                if k < 3 or n % 2 == 1:
                    fwd(k, dy, zm, 1, 0)
                to_sib(k, dy)
            if k == 2:
                x_relay(0)
                x_relay(1)
        x_relay(2)
        for dy in (0, 1, 3, 2):
            got(4, dy)
            to_sib(4, dy)
        x_relay(3)
        arrived(sibB, irec.at[1])
        for r in range(1, 32):
            arrived(WB.at[(z + r // NY) % NZ, (y + r % NY) % NY], srec.at[r])

    def run_b():
        def piece(dz, dy):
            return WB.at[(z + dz) % NZ, (y + dy) % NY]

        def fwd(dz, dy, peer, ddz, ddy):
            p = piece(dz, dy)
            send(p, p, wrec.at[rel(dz + ddz, dy + ddy)], peer, "b")

        def to_sib(dz, dy):
            p = piece(dz, dy)
            send(p, p, srec.at[rel(dz, dy)], sib, "b")

        def got(dz, dy):
            arrived(piece(dz, dy), wrec.at[rel(dz, dy)])

        def z_part(k):
            for dz in ((-k, k) if k < 4 else (4,)):
                got(dz, 0)
                if k < 3 or (k == 3 and dz < 0):
                    fwd(dz, 0, zp if dz < 0 else zm, -1 if dz < 0 else 1, 0)
                fwd(dz, 0, yp, 0, -1)
                fwd(dz, 0, ym, 0, 1)
                to_sib(dz, 0)

        def y_part(k):
            for dz in ((0,) if k == 0 else (-k, k) if k < 4 else (4,)):
                up = k == 0 or (k < 4 and dz > 0)
                got(dz, 3)
                if up:
                    fwd(dz, 3, yp, 0, -1)
                to_sib(dz, 3)
                got(dz, 1)
                if not up:
                    fwd(dz, 1, ym, 0, 1)
                to_sib(dz, 1)

        def d_part(k):
            for dz in ((0,) if k == 0 else (-k, k) if k < 4 else (4,)):
                got(dz, 2)
                to_sib(dz, 2)

        arrived(sibB, irec.at[1])
        fwd(0, 0, zp, -1, 0)
        fwd(0, 0, zm, 1, 0)
        fwd(0, 0, yp, 0, -1)
        fwd(0, 0, ym, 0, 1)
        z_part(1)
        y_part(0)
        z_part(2)
        y_part(1)
        d_part(0)
        z_part(3)
        y_part(2)
        d_part(1)
        x_relay(0)
        x_relay(1)
        z_part(4)
        y_part(3)
        d_part(2)
        y_part(4)
        x_relay(2)
        d_part(3)
        d_part(4)
        x_relay(3)
        arrived(sibA, irec.at[0])
        for r in range(1, 32):
            arrived(WA.at[(z + r // NY) % NZ, (y + r % NY) % NY], srec.at[r])

    for cp in l_small:
        cp.wait()
    lane = lax.broadcasted_iota(jnp.int32, (GRID, HEAD), 1)
    line = lax.broadcasted_iota(jnp.int32, (GRID, HEAD), 0).astype(F32)
    by_row = lane < HEAD // 2
    negative = (lane // 32) % 2 == 0
    freq = freq_v[0:1, :]
    column_angle = line * freq
    column_cos, column_sin = jnp.cos(column_angle), jnp.sin(column_angle)
    first = (s * (ROWS // GRID)).astype(F32)
    row_angle = (lax.broadcasted_iota(jnp.int32, (16, HEAD), 0).astype(F32) + first) * freq
    row_cos, row_sin = jnp.cos(row_angle), jnp.sin(row_angle)
    for r in range(ROWS // GRID):
        COS[r * GRID : (r + 1) * GRID, :] = jnp.where(by_row, row_cos[r : r + 1, :], column_cos)
        sine = jnp.where(by_row, row_sin[r : r + 1, :], column_sin)
        SIN[r * GRID : (r + 1) * GRID, :] = jnp.where(negative, -sine, sine)

    base = len(sent)
    spans = []
    for c, run in ((0, run_a), (1, run_b)):
        @pl.when(core == c)
        def _(run=run):
            run()
            spans.append(sent[base:])
            del sent[base:]
    sent.extend([None] * max(len(span) for span in spans))

    negative = (lax.broadcasted_iota(jnp.int32, (256, HEAD), 1) // 32) % 2 == 0
    row256 = lax.broadcasted_iota(jnp.int32, (256, 1), 0)

    def rotate(u, cosine, sine):
        turned = jnp.where(negative, pltpu.roll(u, 96, 1), pltpu.roll(u, 32, 1))
        return (u * cosine + turned * sine).astype(BF16)

    def weight(ref, c0):
        return ref[:, :, :, c0 : c0 + 256].reshape(WIDTH, 256)

    def project(m):
        rows = slice(256 * m, 256 * m + 256)
        blocks = ORDER[2 * m : 2 * m + 2]
        cosine = jnp.concatenate([COS[b * 128 : b * 128 + 128, :] for b in blocks], 0)
        sine = jnp.concatenate([SIN[b * 128 : b * 128 + 128, :] for b in blocks], 0)
        q = jnp.dot(T[rows, :], weight(WA, 0), preferred_element_type=F32)
        for h in range(2):
            u = rotate(q[:, h * HEAD : (h + 1) * HEAD], cosine, sine)
            for i, b in enumerate(blocks):
                Q[b, h * 128 : (h + 1) * 128, :] = u[i * 128 : (i + 1) * 128]
        kv = jnp.dot(T[rows, :], weight(WA, 256), preferred_element_type=F32)
        k = rotate(kv[:, :HEAD], cosine, sine)
        v = kv[:, HEAD:].astype(BF16)
        for i, b in enumerate(blocks):
            KV[b + 1, :, 0:HEAD] = k[i * 128 : (i + 1) * 128]
            KV[b + 1, :, HEAD:] = v[i * 128 : (i + 1) * 128]
        c_in = jnp.dot(T[rows, :], weight(WB, 0), preferred_element_type=F32)
        before = jnp.dot(T[rows, :], weight(WB, 512), preferred_element_type=F32)
        sec = (before * c_in).astype(BF16)
        for i, b in enumerate(blocks):
            SEC[b] = sec[i * 128 : (i + 1) * 128].astype(F32)
            if m == 0:
                ES[i] = sec[0:16] if i == 0 else sec[240:256]
        after = jnp.dot(T[rows, :], weight(WB, 256), preferred_element_type=F32)
        for i, b in enumerate(blocks):
            GA[b] = after[i * 128 : (i + 1) * 128]

    row128 = lax.broadcasted_iota(jnp.int32, (128, 1), 0)
    taps = taps_v[...].astype(F32)

    def convolve(b):
        sec = SEC[b]
        if b > 0:
            low = SEC[b - 1, 127:128, :]
        else:
            low = jnp.where(s > 0, ER[0].astype(F32)[15:16, :], 0.0)
        if b < 5:
            high = SEC[b + 1, 0:1, :]
        else:
            high = jnp.where(s < NSP - 1, ER[1].astype(F32)[0:1, :], 0.0)
        before = jnp.where(row128 == 0, low, pltpu.roll(sec, 1, 0))
        later = jnp.where(row128 == 127, high, pltpu.roll(sec, 127, 0))
        mix = before * taps[0:1] + sec * taps[1:2] + later * taps[2:3]
        MIX[b * 128 : (b + 1) * 128, 256:512] = (GA[b] * mix).astype(BF16)

    qi = lax.broadcasted_iota(jnp.int32, (256, 384), 0) % 128
    kj = lax.broadcasted_iota(jnp.int32, (256, 384), 1)
    inside = (kj >= qi) & (kj <= qi + 256)
    sink_col = jnp.where(row256 < 128, sink[0], sink[1])

    def attend(b):
        keys = KV[b : b + 3, :, 0:HEAD].reshape(384, HEAD)
        values = KV[b : b + 3, :, HEAD:].reshape(384, HEAD)
        scores = nt_dot(Q[b], keys) * HEAD ** (-0.5)
        valid = inside
        if b == 0:
            valid = valid & ((kj >= 128) | (s > 0))
        if b == 5:
            valid = valid & ((kj < 256) | (s < NSP - 1))
        scores = jnp.where(valid, scores, NEG_BIG)
        top = jnp.maximum(jnp.max(scores, 1, keepdims=True), sink_col)
        w = jnp.exp(scores - top)
        total = jnp.sum(w, 1, keepdims=True) + jnp.exp(sink_col - top)
        probs = (w / total).astype(BF16)
        o = jnp.dot(probs, values, preferred_element_type=F32).astype(BF16)
        rows = slice(b * 128, b * 128 + 128)
        MIX[rows, 0:HEAD] = o[:128]
        MIX[rows, HEAD : 2 * HEAD] = o[128:]

    def halo_send():
        send(KV.at[1], KV.at[7], hrec.at[0], sm)
        send(KV.at[6], KV.at[0], hrec.at[1], sp)
        send(ES.at[0], ER.at[1], hrec.at[2], sm)
        send(ES.at[1], ER.at[0], hrec.at[3], sp)

    def halo_left():
        arrived(KV.at[0], hrec.at[1])
        arrived(ER.at[0], hrec.at[3])

    def halo_right():
        arrived(KV.at[7], hrec.at[0])
        arrived(ER.at[1], hrec.at[2])

    def partial(g, d):
        o = (x + d) % NX
        a = MIX[256 * g : 256 * g + 256, 0:256]
        c = MIX[256 * g : 256 * g + 256, 256:512]
        wa = WA[pl.ds(2 * o, 2), :, :, 512:768].reshape(QUARTER, 256)
        wb = WB[pl.ds(2 * o, 2), :, :, 768:1024].reshape(QUARTER, 256)
        return nt_dot(a, wa) + nt_dot(c, wb)

    def spread_out(g):
        p = partial(g, 2).astype(BF16)
        S2[g, 0] = p[:128]
        S2[g, 1] = p[128:]
        send(S2.at[g, 0], R2.at[g, 0], r2rec.at[2 * g], xp)
        send(S2.at[g, 1], R2.at[g, 1], r2rec.at[2 * g + 1], xm)
        p = partial(g, 1)
        PT[g] = p[:128]
        S1[g, 0, 1] = p[128:].astype(BF16)
        send(S1.at[g, 0, 1], R1.at[g, 0, 1], r1rec.at[4 * g + 1], xp)
        p = partial(g, 3)
        PB[g] = p[128:]
        S1[g, 1, 0] = p[:128].astype(BF16)
        send(S1.at[g, 1, 0], R1.at[g, 1, 0], r1rec.at[4 * g + 2], xm)
        PX[g] = partial(g, 0)

    def sum_relay(g):
        arrived(R2.at[g, 0], r2rec.at[2 * g])
        S1[g, 0, 0] = (PT[g] + R2[g, 0].astype(F32)).astype(BF16)
        send(S1.at[g, 0, 0], R1.at[g, 0, 0], r1rec.at[4 * g], xp)
        arrived(R2.at[g, 1], r2rec.at[2 * g + 1])
        S1[g, 1, 1] = (PB[g] + R2[g, 1].astype(F32)).astype(BF16)
        send(S1.at[g, 1, 1], R1.at[g, 1, 1], r1rec.at[4 * g + 3], xm)

    def local_stats(g):
        for i in range(2):
            for half in range(2):
                arrived(R1.at[g, i, half], r1rec.at[4 * g + 2 * i + half])
        for half in range(2):
            rows = slice(128 * half, 128 * half + 128)
            t = PX[g, rows, :] + R1[g, 0, half].astype(F32) + R1[g, 1, half].astype(F32)
            PX[g, rows, :] = t
            mean = jnp.sum(t, 1, keepdims=True) * (1.0 / QUARTER)
            m2 = jnp.sum(jnp.square(t - mean), 1, keepdims=True)
            lane = lax.broadcasted_iota(jnp.int32, (128, 128), 1)
            both = jnp.where(lane == 0, mean, m2)
            ST[g, 0, half] = jnp.transpose(both)[0:8, :]
        for d, peer, slot in ((1, xp, 3), (3, xm, 1), (2, x2, 2)):
            send(ST.at[g, 0], ST.at[g, slot], strec.at[3 * g + slot - 1], peer)

    def finish(g):
        for slot in (1, 2, 3):
            arrived(ST.at[g, slot], strec.at[3 * g + slot - 1])
        for half in range(2):
            rows = slice(128 * half, 128 * half + 128)
            parts = [ST[g, slot, half] for slot in range(4)]
            means = [p[0:1, :] for p in parts]
            mean = (means[0] + means[1] + means[2] + means[3]) * 0.25
            m2 = sum(p[1:2, :] for p in parts)
            for m in means:
                m2 = m2 + QUARTER * jnp.square(m - mean)
            scale = lax.rsqrt(m2 * (1.0 / WIDTH) + EPS)
            line = lax.broadcasted_iota(jnp.int32, (128, 128), 0)
            columns = jnp.transpose(jnp.where(line == 0, mean, scale))
            normed = (PX[g, rows, :] - columns[:, 0:1]) * columns[:, 1:2] * gain_v[0:1, :]
            OUT[g, rows, :] = normed.astype(BF16)
        cp = pltpu.make_async_copy(OUT.at[g], out.at[pl.ds(256 * g, 256), :], osem.at[g])
        cp.start()
        outs.append(cp)

    outs = []
    x_rest(0)
    x_rest(1)
    project(0)
    halo_send()
    x_rest(2)
    project(1)
    convolve(1)
    attend(1)
    halo_left()
    convolve(0)
    attend(0)
    spread_out(0)
    x_rest(3)
    project(2)
    convolve(2)
    convolve(3)
    attend(2)
    attend(3)
    spread_out(1)
    sum_relay(0)
    convolve(4)
    attend(4)
    halo_right()
    convolve(5)
    attend(5)
    spread_out(2)
    sum_relay(1)
    local_stats(0)
    sum_relay(2)
    finish(0)
    local_stats(1)
    finish(1)
    local_stats(2)
    finish(2)
    for cp in sent:
        if cp is not None:
            cp.wait_send()
    likes = {"a": WA.at[0, 0], "b": WB.at[0, 0], "t": T.at[pl.ds(0, 128), pl.ds(0, QUARTER)]}
    for c, span in enumerate(spans):
        @pl.when(core == c)
        def _(span=span):
            for i, like in enumerate(span):
                copy(likes[like], likes[like], osem.at[0], xp, base + i).wait_send()
    for cp in outs:
        cp.wait()


def body(
    tokens, query_weight, key_projection, value_projection, conv_in_weight, conv_gate_out,
    conv_gate_in, conv_taps, head_sink_logit, out_attn_weight, out_conv_weight, out_gain,
):
    half = HEAD // 2
    inverse = np.float32(THETA) ** (-np.arange(0, half, 2, dtype=np.float32) / np.float32(half))
    freq = jnp.asarray(np.tile(inverse.astype(np.float32), 4)[None, :])
    anywhere = pl.BlockSpec(memory_space=pl.ANY)
    specs = [anywhere] * 13
    specs[8] = pl.BlockSpec(memory_space=pltpu.SMEM)
    dma = pltpu.SemaphoreType.DMA
    return pl.pallas_call(
        kernel,
        out_shape=jax.ShapeDtypeStruct((ROWS, QUARTER), BF16),
        in_specs=specs,
        out_specs=anywhere,
        scratch_shapes=[
            pltpu.VMEM((ROWS, WIDTH), BF16),
            pltpu.VMEM((NZ, NY, 64, CA), BF16),
            pltpu.VMEM((NZ, NY, 64, CB), BF16),
            pltpu.VMEM((8, 128, 256), BF16),
            pltpu.VMEM((6, 256, 128), BF16),
            pltpu.VMEM((6, 128, 256), F32),
            pltpu.VMEM((6, 128, 256), F32),
            pltpu.VMEM((ROWS, QUARTER), BF16),
            pltpu.VMEM((2, 16, 256), BF16),
            pltpu.VMEM((2, 16, 256), BF16),
            pltpu.VMEM((ROWS, HEAD), F32),
            pltpu.VMEM((ROWS, HEAD), F32),
            pltpu.VMEM((3, 2, 128, QUARTER), BF16),
            pltpu.VMEM((3, 128, QUARTER), F32),
            pltpu.VMEM((3, 128, QUARTER), F32),
            pltpu.VMEM((3, 256, QUARTER), F32),
            pltpu.VMEM((3, 2, 2, 128, QUARTER), BF16),
            pltpu.VMEM((3, 2, 128, QUARTER), BF16),
            pltpu.VMEM((3, 2, 2, 128, QUARTER), BF16),
            pltpu.VMEM((3, 4, 2, 8, 128), F32),
            pltpu.VMEM((3, 256, QUARTER), BF16),
            pltpu.VMEM((256, 32), BF16),
            pltpu.VMEM((256, 32), BF16),
            pltpu.VMEM((3, 256), BF16),
            pltpu.VMEM((1, QUARTER), F32),
            pltpu.VMEM((1, HEAD), F32),
            dma((16,)),
            dma((144,)),
            dma((32,)),
            dma((32,)),
            dma((2,)),
            dma((14,)),
            dma((4,)),
            dma((6,)),
            dma((12,)),
            dma((9,)),
            dma((3,)),
        ],
        compiler_params=pltpu.CompilerParams(
            collective_id=0, has_side_effects=True, vmem_limit_bytes=56 * 1024 * 1024
        ),
    )(
        tokens, query_weight, key_projection, value_projection, conv_in_weight, conv_gate_out,
        conv_gate_in, conv_taps, head_sink_logit, out_attn_weight, out_conv_weight,
        out_gain.reshape(1, -1), freq,
    )


def solution(mesh):
    return jax.shard_map(
        body,
        mesh=mesh,
        in_specs=(
            P("sp", "tp"),
            P("sp", "tp"),
            P("sp", "tp"),
            P("sp", "tp"),
            P("sp", "tp"),
            P("sp", "tp"),
            P("sp", "tp"),
            P(None, "tp"),
            P("tp"),
            P("tp", "sp"),
            P("tp", "sp"),
            P("tp"),
        ),
        out_specs=P("sp", "tp"),
        check_vma=False,
    )
```

```python
import functools

import jax
import jax.numpy as jnp
import numpy as np
from jax import lax
from jax.experimental import pallas as pl
from jax.experimental.pallas import tpu as pltpu
from jax.sharding import PartitionSpec as P

MESH = pl.DeviceIdType.MESH
F32 = jnp.float32
BF16 = jnp.bfloat16

HEAD = 128
WINDOW = 128
GRID = 64
NEG_BIG = -1e30
THETA = 10000.0
EPS = 1e-05

NZ, NY, NX, NSP = 8, 4, 4, 64
ROWS = 768
WIDTH = 2048
QUARTER = 512
ORDER = (0, 5, 1, 2, 3, 4)
CHUNKS = ((0, 128, 0), (128, 128, 640), (256, 256, 128), (512, 256, 384))


def nt_dot(a, b):
    return lax.dot_general(a, b, (((1,), (1,)), ((), ())), preferred_element_type=F32)


def kernel(
    tok, qw, kw, vw, cin, cgo, cgi, taps_in, sink, owa, owc, gain_in, freq_in, out,
    T, WA, WB, WC, WD, KV, Q, SEC, GA, MIX, ES, ER, COS, SIN, S2, PT, PB, PX, S1, R2, R1, ST, OUT,
    taps_v, gain_v, freq_v,
    lsem, met, csem, wsem, wrec, srec, irec, xrec, hrec, r2rec, r1rec, strec, osem,
):
    s = lax.axis_index("sp")
    x = lax.axis_index("tp")
    core = s % 2
    chip = s // 2
    y = chip % NY
    z = chip // NY

    def at(zz, yy, cc):
        return ((zz % NZ) * NY + yy % NY) * 2 + cc

    sib = (at(z, y, 1 - core), x)
    yp, ym, y2 = [(at(z, y + d, core), x) for d in (1, 3, 2)]
    zp, zm = [(at(z + d, y, core), x) for d in (1, NZ - 1)]
    xp, xm, x2 = [(s, (x + d) % NX) for d in (1, 3, 2)]
    sp, sm = [((s + d) % NSP, x) for d in (1, NSP - 1)]

    loads = []

    def load(src, dst):
        cp = pltpu.make_async_copy(src, dst, lsem.at[len(loads)])
        cp.start()
        loads.append(cp)
        return cp

    own_cols = pl.ds(pl.multiple_of(x * QUARTER, QUARTER), QUARTER)
    own_rows = pl.ds(pl.multiple_of(core * 32, 32), 32)
    l_w = [
        load(qw, WA.at[z, y, own_rows, pl.ds(0, 256)]),
        load(kw, WA.at[z, y, own_rows, pl.ds(256, 128)]),
        load(vw, WA.at[z, y, own_rows, pl.ds(384, 128)]),
        load(cin, WB.at[z, y, own_rows, pl.ds(0, 256)]),
        load(cgi, WB.at[z, y, own_rows, pl.ds(256, 256)]),
        load(owa, WC.at[z, y, own_rows]),
        load(cgo, WD.at[z, y, own_rows, pl.ds(0, 256)]),
        load(owc, WD.at[z, y, own_rows, pl.ds(256, 256)]),
    ]
    l_t = [
        load(tok.at[pl.ds(src, n), :], T.at[pl.ds(dst, n), own_cols])
        for dst, n, src in CHUNKS
    ]
    l_small = [load(taps_in, taps_v), load(gain_in, gain_v), load(freq_in, freq_v)]

    barrier = pltpu.get_barrier_semaphore()

    def greet(peer):
        pl.semaphore_signal(barrier, inc=1, device_id=peer, device_id_type=MESH)

    greet(sib)
    for d in (1, 3):
        greet((at(z, y, 0), (x + d) % NX))
        greet((at(z, y + d, 1), x))
    for d in (1, NZ - 1):
        greet((at(z + d, y, 1), x))

    @pl.when(core == 0)
    def _():
        greet((at(z, y + 2, 1), x))

    for cp in l_w:
        cp.wait()

    @pl.when(core == 0)
    def _():
        pl.semaphore_wait(barrier, 5)
        pl.semaphore_signal(met, inc=1, device_id=sib, device_id_type=MESH)

    @pl.when(core == 1)
    def _():
        pl.semaphore_wait(met, 1)

    counts = [0, 0, 0, 0]

    def copy(src, dst, rsem, peer, ssem):
        return pltpu.make_async_remote_copy(
            src_ref=src, dst_ref=dst, send_sem=ssem, recv_sem=rsem,
            device_id=peer, device_id_type=MESH,
        )

    def send(src, dst, rsem, peer, ssem):
        copy(src, dst, rsem, peer, ssem).start()

    def send_weights(n, src, rsem, peer):
        i = counts[n]
        counts[n] += 1
        send(src, src, rsem, peer, wsem.at[n // 2, 0 if i < 32 else 1 if i < 60 else 2])

    def sent(ref, ssem):
        copy(ref, ref, osem.at[0], xp, ssem).wait_send()

    def on_core(c, *steps):
        @pl.when(core == c)
        def _():
            for step, *args in steps:
                step(*args)

    def arrived(ref, rsem):
        copy(ref, ref, rsem, xp, csem.at[0]).wait_recv()

    sib_rows = pl.ds(pl.multiple_of((1 - core) * 32, 32), 32)
    W = (WA, WB, WC, WD)
    for n, w in enumerate(W):
        send(w.at[z, y, own_rows], w.at[z, y, own_rows], irec.at[n], sib, csem.at[n])

    def from_sib(n):
        arrived(W[n].at[z, y, sib_rows], irec.at[n])

    def cols(d):
        return pl.ds(pl.multiple_of(((x + d) % NX) * QUARTER, QUARTER), QUARTER)

    def x_send(i):
        dst, n, _ = CHUNKS[i]
        blk = T.at[pl.ds(dst, n), own_cols]
        send(blk, blk, xrec.at[i], xp, csem.at[4])
        send(blk, blk, xrec.at[4 + i], xm, csem.at[4])

    for cp in l_t:
        cp.wait()
    for i in range(3):
        x_send(i)

    @pl.when(core == 1)
    def _():
        pl.semaphore_wait(barrier, 10)
        pl.semaphore_signal(met, inc=1, device_id=sib, device_id_type=MESH)

    @pl.when(core == 0)
    def _():
        pl.semaphore_wait(met, 1)

    RELAY = (
        ((0, 0, 128, 1),),
        ((1, 128, 128, -1),),
        ((2, 256, 128, 1), (2, 384, 128, -1)),
        ((3, 512, 128, 1), (3, 640, 128, -1)),
    )

    def t_chunk(i, d):
        dst, n, _ = CHUNKS[i]
        return T.at[pl.ds(dst, n), cols(d)]

    def x_relay(i):
        for _, r0, n, direction in RELAY[i]:
            if direction == 1:
                arrived(t_chunk(i, 3), xrec.at[i])
                blk = T.at[pl.ds(r0, n), cols(3)]
                send(blk, blk, xrec.at[8 + r0 // 128], xp, csem.at[4])
            else:
                arrived(t_chunk(i, 1), xrec.at[4 + i])
                blk = T.at[pl.ds(r0, n), cols(1)]
                send(blk, blk, xrec.at[8 + r0 // 128], xm, csem.at[4])

    def x_rest(i):
        if i == 0:
            arrived(t_chunk(0, 1), xrec.at[4])
            arrived(T.at[pl.ds(0, 128), cols(2)], xrec.at[8])
        elif i == 1:
            arrived(t_chunk(1, 3), xrec.at[1])
            arrived(T.at[pl.ds(128, 128), cols(2)], xrec.at[9])
        else:
            r0 = CHUNKS[i][0]
            arrived(T.at[pl.ds(r0, 128), cols(2)], xrec.at[8 + r0 // 128])
            arrived(T.at[pl.ds(r0 + 128, 128), cols(2)], xrec.at[9 + r0 // 128])

    def rel(dz, dy):
        return (dz % NZ) * NY + dy % NY

    def piece(n, dz, dy):
        return W[n].at[(z + dz) % NZ, (y + dy) % NY]

    def fwd(n, dz, dy, peer, ddz, ddy):
        p = piece(n, dz, dy)
        send_weights(n, p, wrec.at[n // 2, rel(dz + ddz, dy + ddy)], peer)

    def to_sib(n, dz, dy):
        p = piece(n, dz, dy)
        send_weights(n, p, srec.at[n // 2, 1 if dz == 0 else 0], sib)

    def got(n, dz, dy):
        arrived(piece(n, dz, dy), wrec.at[n // 2, rel(dz, dy)])

    def all_from_sib(n):
        from_sib(n)
        arrived(W[n].at[pl.ds(0, 7)], srec.at[n // 2, 0])
        arrived(W[n].at[0, pl.ds(0, 3)], srec.at[n // 2, 1])

    def a_ysend(n):
        from_sib(n)
        fwd(n, 0, 0, yp, 0, -1)
        fwd(n, 0, 0, ym, 0, 1)
        fwd(n, 0, 0, y2, 0, 2)

    def a_zsend(n):
        fwd(n, 0, 0, zp, -1, 0)
        fwd(n, 0, 0, zm, 1, 0)

    def a_y(n):
        for dy in (1, 3, 2):
            got(n, 0, dy)
            fwd(n, 0, dy, zp, -1, 0)
            fwd(n, 0, dy, zm, 1, 0)
            to_sib(n, 0, dy)

    def a_hop(n, k):
        for i, dy in enumerate((0, 1, 3, 2)):
            for dz in (-k, k) if k < 4 else (4,):
                got(n, dz, dy)
                if dz < 0 and (k < 3 or i % 2 == 0):
                    fwd(n, dz, dy, zp, -1, 0)
                if 0 < dz < 4 and (k < 3 or i % 2 == 1):
                    fwd(n, dz, dy, zm, 1, 0)
                to_sib(n, dz, dy)

    def ring(k):
        return (0,) if k == 0 else (-k, k) if k < 4 else (4,)

    def b_start(n):
        from_sib(n)
        fwd(n, 0, 0, zp, -1, 0)
        fwd(n, 0, 0, zm, 1, 0)

    def b_z(n, k):
        for dz in ring(k):
            got(n, dz, 0)
            if dz < 0:
                fwd(n, dz, 0, zp, -1, 0)
            elif k < 3:
                fwd(n, dz, 0, zm, 1, 0)
            to_sib(n, dz, 0)

    def b_zy(n, k):
        for dz in ring(k):
            fwd(n, dz, 0, yp, 0, -1)
            fwd(n, dz, 0, ym, 0, 1)

    def b_y(n, k):
        for dz in ring(k):
            up = k == 0 or 0 < dz < 4
            got(n, dz, 3)
            if up:
                fwd(n, dz, 3, yp, 0, -1)
            to_sib(n, dz, 3)
            got(n, dz, 1)
            if not up:
                fwd(n, dz, 1, ym, 0, 1)
            to_sib(n, dz, 1)

    def b_d(n, k):
        for dz in ring(k):
            got(n, dz, 2)
            to_sib(n, dz, 2)

    for cp in l_small:
        cp.wait()
    lane = lax.broadcasted_iota(jnp.int32, (GRID, HEAD), 1)
    line = lax.broadcasted_iota(jnp.int32, (GRID, HEAD), 0).astype(F32)
    by_row = lane < HEAD // 2
    negative = (lane // 32) % 2 == 0
    freq = freq_v[0:1, :]
    column_angle = line * freq
    column_cos, column_sin = jnp.cos(column_angle), jnp.sin(column_angle)
    first = (s * (ROWS // GRID)).astype(F32)
    row_angle = (lax.broadcasted_iota(jnp.int32, (16, HEAD), 0).astype(F32) + first) * freq
    row_cos, row_sin = jnp.cos(row_angle), jnp.sin(row_angle)
    for r in range(ROWS // GRID):
        COS[r * GRID : (r + 1) * GRID, :] = jnp.where(by_row, row_cos[r : r + 1, :], column_cos)
        sine = jnp.where(by_row, row_sin[r : r + 1, :], column_sin)
        SIN[r * GRID : (r + 1) * GRID, :] = jnp.where(negative, -sine, sine)

    negative = (lax.broadcasted_iota(jnp.int32, (256, HEAD), 1) // 32) % 2 == 0
    row256 = lax.broadcasted_iota(jnp.int32, (256, 1), 0)

    def rotate(u, cosine, sine):
        turned = jnp.where(negative, pltpu.roll(u, 96, 1), pltpu.roll(u, 32, 1))
        return (u * cosine + turned * sine).astype(BF16)

    def weight(ref, c0):
        return ref[:, :, :, c0 : c0 + 256].reshape(WIDTH, 256)

    def project(m):
        rows = slice(256 * m, 256 * m + 256)
        blocks = ORDER[2 * m : 2 * m + 2]
        cosine = jnp.concatenate([COS[b * 128 : b * 128 + 128, :] for b in blocks], 0)
        sine = jnp.concatenate([SIN[b * 128 : b * 128 + 128, :] for b in blocks], 0)
        q = jnp.dot(T[rows, :], weight(WA, 0), preferred_element_type=F32)
        for h in range(2):
            u = rotate(q[:, h * HEAD : (h + 1) * HEAD], cosine, sine)
            for i, b in enumerate(blocks):
                Q[b, h * 128 : (h + 1) * 128, :] = u[i * 128 : (i + 1) * 128]
        kv = jnp.dot(T[rows, :], weight(WA, 256), preferred_element_type=F32)
        k = rotate(kv[:, :HEAD], cosine, sine)
        v = kv[:, HEAD:].astype(BF16)
        for i, b in enumerate(blocks):
            KV[b + 1, :, 0:HEAD] = k[i * 128 : (i + 1) * 128]
            KV[b + 1, :, HEAD:] = v[i * 128 : (i + 1) * 128]

    def project_conv(m):
        rows = slice(256 * m, 256 * m + 256)
        blocks = ORDER[2 * m : 2 * m + 2]
        c_in = jnp.dot(T[rows, :], weight(WB, 0), preferred_element_type=F32)
        before = jnp.dot(T[rows, :], weight(WB, 256), preferred_element_type=F32)
        sec = (before * c_in).astype(BF16)
        for i, b in enumerate(blocks):
            SEC[b] = sec[i * 128 : (i + 1) * 128].astype(F32)
            if m == 0:
                ES[i] = sec[0:16] if i == 0 else sec[240:256]
        after = jnp.dot(T[rows, :], weight(WD, 0), preferred_element_type=F32)
        for i, b in enumerate(blocks):
            GA[b] = after[i * 128 : (i + 1) * 128]

    row128 = lax.broadcasted_iota(jnp.int32, (128, 1), 0)
    taps = taps_v[...].astype(F32)

    def convolve(b):
        sec = SEC[b]
        if b > 0:
            low = SEC[b - 1, 127:128, :]
        else:
            low = jnp.where(s > 0, ER[0].astype(F32)[15:16, :], 0.0)
        if b < 5:
            high = SEC[b + 1, 0:1, :]
        else:
            high = jnp.where(s < NSP - 1, ER[1].astype(F32)[0:1, :], 0.0)
        before = jnp.where(row128 == 0, low, pltpu.roll(sec, 1, 0))
        later = jnp.where(row128 == 127, high, pltpu.roll(sec, 127, 0))
        mix = before * taps[0:1] + sec * taps[1:2] + later * taps[2:3]
        MIX[b * 128 : (b + 1) * 128, 256:512] = (GA[b] * mix).astype(BF16)

    qi = lax.broadcasted_iota(jnp.int32, (256, 384), 0) % 128
    kj = lax.broadcasted_iota(jnp.int32, (256, 384), 1)
    inside = (kj >= qi) & (kj <= qi + 256)
    sink_col = jnp.where(row256 < 128, sink[0], sink[1])

    def attend(b):
        keys = KV[b : b + 3, :, 0:HEAD].reshape(384, HEAD)
        values = KV[b : b + 3, :, HEAD:].reshape(384, HEAD)
        scores = nt_dot(Q[b], keys) * HEAD ** (-0.5)
        valid = inside
        if b == 0:
            valid = valid & ((kj >= 128) | (s > 0))
        if b == 5:
            valid = valid & ((kj < 256) | (s < NSP - 1))
        scores = jnp.where(valid, scores, NEG_BIG)
        top = jnp.maximum(jnp.max(scores, 1, keepdims=True), sink_col)
        w = jnp.exp(scores - top)
        total = jnp.sum(w, 1, keepdims=True) + jnp.exp(sink_col - top)
        probs = (w / total).astype(BF16)
        o = jnp.dot(probs, values, preferred_element_type=F32).astype(BF16)
        rows = slice(b * 128, b * 128 + 128)
        MIX[rows, 0:HEAD] = o[:128]
        MIX[rows, HEAD : 2 * HEAD] = o[128:]

    def halo_send():
        send(KV.at[1], KV.at[7], hrec.at[0], sm, csem.at[5])
        send(KV.at[6], KV.at[0], hrec.at[1], sp, csem.at[5])

    def edge_send():
        send(ES.at[0], ER.at[1], hrec.at[2], sm, csem.at[6])
        send(ES.at[1], ER.at[0], hrec.at[3], sp, csem.at[6])

    def halo_left():
        arrived(KV.at[0], hrec.at[1])

    def edge_left():
        arrived(ER.at[0], hrec.at[3])

    def halo_right():
        arrived(KV.at[7], hrec.at[0])
        arrived(ER.at[1], hrec.at[2])

    def partial(g, d):
        o = (x + d) % NX
        a = MIX[256 * g : 256 * g + 256, 0:256]
        c = MIX[256 * g : 256 * g + 256, 256:512]
        wa = WC[pl.ds(2 * o, 2)].reshape(QUARTER, 256)
        wb = WD[pl.ds(2 * o, 2), :, :, 256:512].reshape(QUARTER, 256)
        return nt_dot(a, wa) + nt_dot(c, wb)

    def spread_out(g):
        p = partial(g, 2).astype(BF16)
        S2[g, 0] = p[:128]
        S2[g, 1] = p[128:]
        send(S2.at[g, 0], R2.at[g, 0], r2rec.at[2 * g], xp, csem.at[7])
        send(S2.at[g, 1], R2.at[g, 1], r2rec.at[2 * g + 1], xm, csem.at[7])
        p = partial(g, 1)
        PT[g] = p[:128]
        S1[g, 0, 1] = p[128:].astype(BF16)
        send(S1.at[g, 0, 1], R1.at[g, 0, 1], r1rec.at[g], xp, csem.at[8])
        p = partial(g, 3)
        PB[g] = p[128:]
        S1[g, 1, 0] = p[:128].astype(BF16)
        send(S1.at[g, 1, 0], R1.at[g, 1, 0], r1rec.at[g], xm, csem.at[8])
        PX[g] = partial(g, 0)

    def sum_relay(g):
        arrived(R2.at[g, 0], r2rec.at[2 * g])
        S1[g, 0, 0] = (PT[g] + R2[g, 0].astype(F32)).astype(BF16)
        send(S1.at[g, 0, 0], R1.at[g, 0, 0], r1rec.at[g], xp, csem.at[8])
        arrived(R2.at[g, 1], r2rec.at[2 * g + 1])
        S1[g, 1, 1] = (PB[g] + R2[g, 1].astype(F32)).astype(BF16)
        send(S1.at[g, 1, 1], R1.at[g, 1, 1], r1rec.at[g], xm, csem.at[8])

    def local_stats(g):
        arrived(R1.at[g], r1rec.at[g])
        for half in range(2):
            rows = slice(128 * half, 128 * half + 128)
            t = PX[g, rows, :] + R1[g, 0, half].astype(F32) + R1[g, 1, half].astype(F32)
            PX[g, rows, :] = t
            mean = jnp.sum(t, 1, keepdims=True) * (1.0 / QUARTER)
            m2 = jnp.sum(jnp.square(t - mean), 1, keepdims=True)
            lane = lax.broadcasted_iota(jnp.int32, (128, 128), 1)
            both = jnp.where(lane == 0, mean, m2)
            ST[g, 0, half] = jnp.transpose(both)[0:8, :]
        for d, peer, slot in ((1, xp, 3), (3, xm, 1), (2, x2, 2)):
            send(ST.at[g, 0], ST.at[g, slot], strec.at[g], peer, csem.at[9])

    def finish(g):
        arrived(ST.at[g, pl.ds(1, 3)], strec.at[g])
        for half in range(2):
            rows = slice(128 * half, 128 * half + 128)
            parts = [ST[g, slot, half] for slot in range(4)]
            means = [p[0:1, :] for p in parts]
            mean = (means[0] + means[1] + means[2] + means[3]) * 0.25
            m2 = sum(p[1:2, :] for p in parts)
            for m in means:
                m2 = m2 + QUARTER * jnp.square(m - mean)
            scale = lax.rsqrt(m2 * (1.0 / WIDTH) + EPS)
            line = lax.broadcasted_iota(jnp.int32, (128, 128), 0)
            columns = jnp.transpose(jnp.where(line == 0, mean, scale))
            normed = (PX[g, rows, :] - columns[:, 0:1]) * columns[:, 1:2] * gain_v[0:1, :]
            OUT[g, rows, :] = normed.astype(BF16)
        cp = pltpu.make_async_copy(OUT.at[g], out.at[pl.ds(256 * g, 256), :], osem.at[g])
        cp.start()
        outs.append(cp)

    outs = []
    on_core(
        0,
        (a_ysend, 0), (a_zsend, 0), (a_ysend, 2), (a_zsend, 2), (a_y, 0), (a_hop, 0, 1),
        (x_relay, 0), (x_relay, 1), (x_send, 3),
        (a_y, 2), (a_hop, 0, 2), (a_hop, 2, 1), (x_relay, 2),
        (a_hop, 0, 3), (a_hop, 2, 2), (a_hop, 0, 4), (x_relay, 3),
    )
    on_core(
        1,
        (b_start, 1), (b_zy, 1, 0), (b_start, 3),
        (b_z, 1, 1), (b_zy, 1, 1), (b_zy, 3, 0), (b_z, 3, 1), (b_zy, 3, 1),
        (b_z, 1, 2), (b_zy, 1, 2), (b_y, 1, 0), (b_z, 3, 2), (b_zy, 3, 2), (b_y, 3, 0), (b_y, 1, 1),
        (x_relay, 0), (x_relay, 1), (x_send, 3),
        (b_z, 1, 3), (b_zy, 1, 3), (b_y, 3, 1), (b_z, 3, 3), (b_zy, 3, 3),
        (b_d, 1, 0), (b_d, 3, 0), (b_y, 1, 2), (b_d, 1, 1), (b_y, 3, 2),
        (b_z, 1, 4), (b_zy, 1, 4), (b_d, 3, 1), (b_z, 3, 4), (b_zy, 3, 4),
        (x_relay, 2), (b_y, 1, 3), (b_y, 3, 3), (b_d, 1, 2), (b_d, 3, 2), (b_y, 1, 4), (b_y, 3, 4),
        (x_relay, 3), (all_from_sib, 0),
    )
    x_rest(0)
    x_rest(1)
    project(0)
    halo_send()
    on_core(0, (a_hop, 2, 3))
    on_core(1, (b_d, 1, 3), (b_d, 3, 3))
    x_rest(2)
    project(1)
    on_core(0, (a_hop, 2, 4))
    on_core(1, (b_d, 1, 4), (b_d, 3, 4))
    attend(1)
    halo_left()
    attend(0)
    on_core(0, (all_from_sib, 1), (all_from_sib, 3))
    on_core(1, (all_from_sib, 2))
    project_conv(0)
    edge_send()
    project_conv(1)
    convolve(1)
    edge_left()
    convolve(0)
    spread_out(0)
    x_rest(3)
    project(2)
    project_conv(2)
    convolve(2)
    convolve(3)
    attend(2)
    attend(3)
    spread_out(1)
    sum_relay(0)
    convolve(4)
    attend(4)
    halo_right()
    convolve(5)
    attend(5)
    spread_out(2)
    sum_relay(1)
    local_stats(0)
    sum_relay(2)
    local_stats(1)
    local_stats(2)
    finish(0)
    finish(1)
    finish(2)
    assert counts == [62] * 4
    for n, w in enumerate(W):
        sent(w.at[z, y, own_rows], csem.at[n])

        @pl.when(core == n % 2)
        def _(n=n, w=w):
            sent(w, wsem.at[n // 2, 0])
            sent(w.at[pl.ds(0, 7)], wsem.at[n // 2, 1])
            sent(w.at[0, pl.ds(0, 2)], wsem.at[n // 2, 2])
    sent(T.at[pl.ds(0, 576)], csem.at[4])
    sent(KV.at[pl.ds(0, 2)], csem.at[5])
    sent(ES, csem.at[6])
    sent(S2, csem.at[7])
    sent(S1, csem.at[8])
    sent(ST.at[:, pl.ds(0, 3)], csem.at[9])
    for cp in outs:
        cp.wait()


def body(
    tokens, query_weight, key_projection, value_projection, conv_in_weight, conv_gate_out,
    conv_gate_in, conv_taps, head_sink_logit, out_attn_weight, out_conv_weight, out_gain,
):
    half = HEAD // 2
    inverse = np.float32(THETA) ** (-np.arange(0, half, 2, dtype=np.float32) / np.float32(half))
    freq = jnp.asarray(np.tile(inverse.astype(np.float32), 4)[None, :])
    anywhere = pl.BlockSpec(memory_space=pl.ANY)
    specs = [anywhere] * 13
    specs[8] = pl.BlockSpec(memory_space=pltpu.SMEM)
    dma = pltpu.SemaphoreType.DMA
    return pl.pallas_call(
        kernel,
        out_shape=jax.ShapeDtypeStruct((ROWS, QUARTER), BF16),
        in_specs=specs,
        out_specs=anywhere,
        scratch_shapes=[
            pltpu.VMEM((ROWS, WIDTH), BF16),
            pltpu.VMEM((NZ, NY, 64, 512), BF16),
            pltpu.VMEM((NZ, NY, 64, 512), BF16),
            pltpu.VMEM((NZ, NY, 64, 256), BF16),
            pltpu.VMEM((NZ, NY, 64, 512), BF16),
            pltpu.VMEM((8, 128, 256), BF16),
            pltpu.VMEM((6, 256, 128), BF16),
            pltpu.VMEM((6, 128, 256), F32),
            pltpu.VMEM((6, 128, 256), F32),
            pltpu.VMEM((ROWS, QUARTER), BF16),
            pltpu.VMEM((2, 16, 256), BF16),
            pltpu.VMEM((2, 16, 256), BF16),
            pltpu.VMEM((ROWS, HEAD), F32),
            pltpu.VMEM((ROWS, HEAD), F32),
            pltpu.VMEM((3, 2, 128, QUARTER), BF16),
            pltpu.VMEM((3, 128, QUARTER), F32),
            pltpu.VMEM((3, 128, QUARTER), F32),
            pltpu.VMEM((3, 256, QUARTER), F32),
            pltpu.VMEM((3, 2, 2, 128, QUARTER), BF16),
            pltpu.VMEM((3, 2, 128, QUARTER), BF16),
            pltpu.VMEM((3, 2, 2, 128, QUARTER), BF16),
            pltpu.VMEM((3, 4, 2, 8, 128), F32),
            pltpu.VMEM((3, 256, QUARTER), BF16),
            pltpu.VMEM((3, 256), BF16),
            pltpu.VMEM((1, QUARTER), F32),
            pltpu.VMEM((1, HEAD), F32),
            dma((16,)),
            pltpu.SemaphoreType.REGULAR,
            dma((10,)),
            dma((2, 3)),
            dma((2, 32)),
            dma((2, 2)),
            dma((4,)),
            dma((14,)),
            dma((4,)),
            dma((6,)),
            dma((3,)),
            dma((3,)),
            dma((3,)),
        ],
        compiler_params=pltpu.CompilerParams(
            collective_id=0, has_side_effects=True, vmem_limit_bytes=56 * 1024 * 1024
        ),
    )(
        tokens, query_weight, key_projection, value_projection, conv_in_weight, conv_gate_out,
        conv_gate_in, conv_taps, head_sink_logit, out_attn_weight.T, out_conv_weight.T,
        out_gain.reshape(1, -1), freq,
    )


def solution(mesh):
    return jax.shard_map(
        body,
        mesh=mesh,
        in_specs=(
            P("sp", "tp"),
            P("sp", "tp"),
            P("sp", "tp"),
            P("sp", "tp"),
            P("sp", "tp"),
            P("sp", "tp"),
            P("sp", "tp"),
            P(None, "tp"),
            P("tp"),
            P("tp", "sp"),
            P("tp", "sp"),
            P("tp"),
        ),
        out_specs=P("sp", "tp"),
        check_vma=False,
    )
```

```python
import functools

import jax
import jax.numpy as jnp
import numpy as np
from jax import lax
from jax.experimental import pallas as pl
from jax.experimental.pallas import tpu as pltpu
from jax.sharding import PartitionSpec as P

MESH = pl.DeviceIdType.MESH
F32 = jnp.float32
BF16 = jnp.bfloat16

HEAD = 128
WINDOW = 128
GRID = 64
NEG_BIG = -1e30
THETA = 10000.0
EPS = 1e-05

NZ, NY, NX, NSP = 8, 4, 4, 64
ROWS = 768
WIDTH = 2048
QUARTER = 512
ORDER = (0, 5, 1, 2, 3, 4)
ICS = {0: 1, 1: 3, 3: 8}
CHUNKS = ((0, 128, 0), (128, 128, 640), (256, 256, 128), (512, 256, 384))


def nt_dot(a, b):
    return lax.dot_general(a, b, (((1,), (1,)), ((), ())), preferred_element_type=F32)


def kernel(
    tok, qw, kw, vw, cin, cgo, cgi, taps_in, sink_in, owa, owc, gain_in, freq_in, out,
    T, WA, WB, WD, WOA, WOC, OWN, KV, Q, SEC, GA, MA, MC, ES, ER, COS, SIN, PX, ST,
    taps_v, gain_v, freq_v, sink,
    lsem, met, csem, wsem, wrec, srec, irec, xrec, hrec, mixrec, strec, osem, worec, wozrec, wozsem, woyrec, wosend, wosib,
):
    s = lax.axis_index("sp")
    x = lax.axis_index("tp")
    core = s % 2
    chip = s // 2
    y = chip % NY
    z = chip // NY

    def at(zz, yy, cc):
        return ((zz % NZ) * NY + yy % NY) * 2 + cc

    sib = (at(z, y, 1 - core), x)
    yp, ym, y2 = [(at(z, y + d, core), x) for d in (1, 3, 2)]
    zp, zm = [(at(z + d, y, core), x) for d in (1, NZ - 1)]
    xp, xm, x2 = [(s, (x + d) % NX) for d in (1, 3, 2)]
    sp, sm = [((s + d) % NSP, x) for d in (1, NSP - 1)]

    loads = []

    def load(src, dst):
        cp = pltpu.make_async_copy(src, dst, lsem.at[len(loads)])
        cp.start()
        loads.append(cp)
        return cp

    own_cols = pl.ds(pl.multiple_of(x * QUARTER, QUARTER), QUARTER)
    own_rows = pl.ds(pl.multiple_of(core * 32, 32), 32)
    l_w = [
        load(qw, WA.at[z, y, own_rows, pl.ds(0, 256)]),
        load(kw, WA.at[z, y, own_rows, pl.ds(256, 128)]),
        load(vw, WA.at[z, y, own_rows, pl.ds(384, 128)]),
        load(cin, WB.at[z, y, own_rows, pl.ds(0, 256)]),
        load(cgi, WB.at[z, y, own_rows, pl.ds(256, 256)]),
        load(cgo, WD.at[z, y, own_rows]),
        load(owa, OWN.at[0]),
        load(owc, OWN.at[1]),
    ]
    l_t = [
        load(tok.at[pl.ds(src, n), :], T.at[pl.ds(dst, n), own_cols])
        for dst, n, src in CHUNKS
    ]
    l_small = [load(taps_in, taps_v), load(gain_in, gain_v), load(freq_in, freq_v), load(sink_in, sink)]

    barrier = pltpu.get_barrier_semaphore()

    def greet(peer):
        pl.semaphore_signal(barrier, inc=1, device_id=peer, device_id_type=MESH)

    greet(sib)
    for d in (1, 3):
        greet((at(z, y, 0), (x + d) % NX))
        greet((at(z, y + d, 1), x))
    for d in (1, NZ - 1):
        greet((at(z + d, y, 1), x))

    @pl.when(core == 0)
    def _():
        greet((at(z, y + 2, 1), x))

    for cp in l_w:
        cp.wait()

    @pl.when(core == 0)
    def _():
        pl.semaphore_wait(barrier, 5)
        pl.semaphore_signal(met, inc=1, device_id=sib, device_id_type=MESH)

    @pl.when(core == 1)
    def _():
        pl.semaphore_wait(met, 1)

    counts = {0: 0, 1: 0, 3: 0}

    def copy(src, dst, rsem, peer, ssem):
        return pltpu.make_async_remote_copy(
            src_ref=src, dst_ref=dst, send_sem=ssem, recv_sem=rsem,
            device_id=peer, device_id_type=MESH,
        )

    def send(src, dst, rsem, peer, ssem):
        copy(src, dst, rsem, peer, ssem).start()

    def send_weights(n, src, rsem, peer):
        i = counts[n]
        counts[n] += 1
        send(src, src, rsem, peer, wsem.at[n // 2, 0 if i < 32 else 1 if i < 60 else 2])

    def sent(ref, ssem):
        copy(ref, ref, osem.at[0], xp, ssem).wait_send()

    def on_core(c, *steps):
        @pl.when(core == c)
        def _():
            for step, *args in steps:
                step(*args)

    def arrived(ref, rsem):
        copy(ref, ref, rsem, xp, csem.at[0]).wait_recv()

    sib_rows = pl.ds(pl.multiple_of((1 - core) * 32, 32), 32)
    W = {0: WA, 1: WB, 3: WD}
    for n, w in W.items():
        send(w.at[z, y, own_rows], w.at[z, y, own_rows], irec.at[n], sib, csem.at[ICS[n]])

    def from_sib(n):
        arrived(W[n].at[z, y, sib_rows], irec.at[n])

    def cols(d):
        return pl.ds(pl.multiple_of(((x + d) % NX) * QUARTER, QUARTER), QUARTER)

    def x_send(i):
        dst, n, _ = CHUNKS[i]
        blk = T.at[pl.ds(dst, n), own_cols]
        send(blk, blk, xrec.at[i], xp, csem.at[4])
        send(blk, blk, xrec.at[4 + i], xm, csem.at[4])

    for cp in l_t:
        cp.wait()
    for i in range(3):
        x_send(i)

    @pl.when(core == 1)
    def _():
        pl.semaphore_wait(barrier, 10)
        pl.semaphore_signal(met, inc=1, device_id=sib, device_id_type=MESH)

    @pl.when(core == 0)
    def _():
        pl.semaphore_wait(met, 1)

    RELAY = (
        ((0, 0, 128, 1),),
        ((1, 128, 128, -1),),
        ((2, 256, 128, 1), (2, 384, 128, -1)),
        ((3, 512, 128, 1), (3, 640, 128, -1)),
    )

    def t_chunk(i, d):
        dst, n, _ = CHUNKS[i]
        return T.at[pl.ds(dst, n), cols(d)]

    def x_relay(i):
        for _, r0, n, direction in RELAY[i]:
            if direction == 1:
                arrived(t_chunk(i, 3), xrec.at[i])
                blk = T.at[pl.ds(r0, n), cols(3)]
                send(blk, blk, xrec.at[8 + r0 // 128], xp, csem.at[4])
            else:
                arrived(t_chunk(i, 1), xrec.at[4 + i])
                blk = T.at[pl.ds(r0, n), cols(1)]
                send(blk, blk, xrec.at[8 + r0 // 128], xm, csem.at[4])

    def x_rest(i):
        if i == 0:
            arrived(t_chunk(0, 1), xrec.at[4])
            arrived(T.at[pl.ds(0, 128), cols(2)], xrec.at[8])
        elif i == 1:
            arrived(t_chunk(1, 3), xrec.at[1])
            arrived(T.at[pl.ds(128, 128), cols(2)], xrec.at[9])
        else:
            r0 = CHUNKS[i][0]
            arrived(T.at[pl.ds(r0, 128), cols(2)], xrec.at[8 + r0 // 128])
            arrived(T.at[pl.ds(r0 + 128, 128), cols(2)], xrec.at[9 + r0 // 128])

    def rel(dz, dy):
        return (dz % NZ) * NY + dy % NY

    def piece(n, dz, dy):
        return W[n].at[(z + dz) % NZ, (y + dy) % NY]

    def fwd(n, dz, dy, peer, ddz, ddy):
        p = piece(n, dz, dy)
        send_weights(n, p, wrec.at[n // 2, rel(dz + ddz, dy + ddy)], peer)

    def to_sib(n, dz, dy):
        p = piece(n, dz, dy)
        send_weights(n, p, srec.at[n // 2, 1 if dz == 0 else 0], sib)

    def got(n, dz, dy):
        arrived(piece(n, dz, dy), wrec.at[n // 2, rel(dz, dy)])

    def all_from_sib(n):
        from_sib(n)
        arrived(W[n].at[pl.ds(0, 7)], srec.at[n // 2, 0])
        arrived(W[n].at[0, pl.ds(0, 3)], srec.at[n // 2, 1])

    def a_ysend(n):
        from_sib(n)
        fwd(n, 0, 0, yp, 0, -1)
        fwd(n, 0, 0, ym, 0, 1)
        fwd(n, 0, 0, y2, 0, 2)

    def a_zsend(n):
        fwd(n, 0, 0, zp, -1, 0)
        fwd(n, 0, 0, zm, 1, 0)

    def a_y(n):
        for dy in (1, 3, 2):
            got(n, 0, dy)
            fwd(n, 0, dy, zp, -1, 0)
            fwd(n, 0, dy, zm, 1, 0)
            to_sib(n, 0, dy)

    def a_hop(n, k):
        for i, dy in enumerate((0, 1, 3, 2)):
            for dz in (-k, k) if k < 4 else (4,):
                got(n, dz, dy)
                if dz < 0 and (k < 3 or i % 2 == 0):
                    fwd(n, dz, dy, zp, -1, 0)
                if 0 < dz < 4 and (k < 3 or i % 2 == 1):
                    fwd(n, dz, dy, zm, 1, 0)
                to_sib(n, dz, dy)

    def ring(k):
        return (0,) if k == 0 else (-k, k) if k < 4 else (4,)

    def b_start(n):
        from_sib(n)
        fwd(n, 0, 0, zp, -1, 0)
        fwd(n, 0, 0, zm, 1, 0)

    def b_z(n, k):
        for dz in ring(k):
            got(n, dz, 0)
            if dz < 0:
                fwd(n, dz, 0, zp, -1, 0)
            elif k < 3:
                fwd(n, dz, 0, zm, 1, 0)
            to_sib(n, dz, 0)

    def b_zy(n, k):
        for dz in ring(k):
            fwd(n, dz, 0, yp, 0, -1)
            fwd(n, dz, 0, ym, 0, 1)

    def b_y(n, k):
        for dz in ring(k):
            up = k == 0 or 0 < dz < 4
            got(n, dz, 3)
            if up:
                fwd(n, dz, 3, yp, 0, -1)
            to_sib(n, dz, 3)
            got(n, dz, 1)
            if not up:
                fwd(n, dz, 1, ym, 0, 1)
            to_sib(n, dz, 1)

    def b_d(n, k):
        for dz in ring(k):
            got(n, dz, 2)
            to_sib(n, dz, 2)

    WO = (WOA, WOC)
    owner = z // 2
    place = (z + NZ - 2 * x) % NZ
    right = (place >= 1) & (place <= 4)
    dist = jnp.where(right, place - 1, (NZ - place) % NZ)
    u1 = jnp.where(right, 1, 0)
    u2 = 1 - u1
    onward = (at(z + jnp.where(right, 1, NZ - 1), y, core), x)
    back = (at(z + jnp.where(right, NZ - 1, 1), y, core), x)

    def wo_x():
        for h in range(2):
            here = (owner == x) & (core == h)

            @pl.when(here)
            def _(h=h):
                WO[h][z % 2, y, x, own_rows, :] = OWN[h]

            @pl.when(jnp.logical_not(here))
            def _(h=h):
                send(
                    OWN.at[h], WO[h].at[z % 2, y, x, own_rows], worec.at[(x + NX - owner) % NX],
                    (at(z, y, h), owner), csem.at[2 * h],
                )

    def wo_x_sent():
        for h in range(2):
            @pl.when(jnp.logical_not((owner == x) & (core == h)))
            def _(h=h):
                sent(OWN.at[h], csem.at[2 * h])

    def wo_share(h, u):
        unit = WO[h].at[u, y]
        send(unit, unit, woyrec.at[0, u], yp, wosend.at[0])
        send(unit, unit, woyrec.at[1, u], ym, wosend.at[0])
        send(unit, unit, wosib.at[0], sib, wosend.at[2])

    def wo_slot(h, k):
        if k < 4:
            @pl.when(dist == k)
            def _():
                unit = WO[h].at[u1, y]
                if k == 0:
                    arrived(WO[h].at[z % 2, y, x, sib_rows], worec.at[0])
                    for d in (1, 2, 3):
                        arrived(WO[h].at[z % 2, y, (x + d) % NX], worec.at[d])
                    send(unit, unit, wozrec.at[1], back, wozsem.at[1])
                else:
                    arrived(unit, wozrec.at[0])
                if k < 3:
                    send(unit, unit, wozrec.at[0], onward, wozsem.at[0])
                wo_share(h, u1)
        if k > 0:
            @pl.when(dist == k - 1)
            def _():
                unit = WO[h].at[u2, y]
                arrived(unit, wozrec.at[1])
                if k < 4:
                    send(unit, unit, wozrec.at[1], onward, wozsem.at[2])
                wo_share(h, u2)

    def wo_y(h):
        for u in range(2):
            for d, o in ((3, 0), (1, 1)):
                unit = WO[h].at[u, (y + d) % NY]
                arrived(unit, woyrec.at[o, u])
                if u == o:
                    send(unit, unit, woyrec.at[2, u], yp if u == 0 else ym, wosend.at[1])
                send(unit, unit, wosib.at[0], sib, wosend.at[2])

    def wo_d(h):
        for u in range(2):
            unit = WO[h].at[u, (y + 2) % NY]
            arrived(unit, woyrec.at[2, u])
            send(unit, unit, wosib.at[0], sib, wosend.at[2])

    def wo_end(h):
        arrived(WO[1 - h], wosib.at[0])

    def wo_sent():
        unit = WOA.at[0, 0]
        sent(WOA.at[0], wosend.at[0])
        sent(WOA.at[0, pl.ds(0, 2)], wosend.at[1])
        sent(WOA, wosend.at[2])

        @pl.when(dist < 3)
        def _():
            sent(unit, wozsem.at[0])

        @pl.when(dist < 4)
        def _():
            @pl.when(dist < 3)
            def _():
                sent(unit, wozsem.at[2])

        @pl.when(dist == 0)
        def _():
            sent(unit, wozsem.at[1])

    for cp in l_small:
        cp.wait()
    lane = lax.broadcasted_iota(jnp.int32, (GRID, HEAD), 1)
    line = lax.broadcasted_iota(jnp.int32, (GRID, HEAD), 0).astype(F32)
    by_row = lane < HEAD // 2
    negative = (lane // 32) % 2 == 0
    freq = freq_v[0:1, :]
    column_angle = line * freq
    column_cos, column_sin = jnp.cos(column_angle), jnp.sin(column_angle)
    first = (s * (ROWS // GRID)).astype(F32)
    row_angle = (lax.broadcasted_iota(jnp.int32, (16, HEAD), 0).astype(F32) + first) * freq
    row_cos, row_sin = jnp.cos(row_angle), jnp.sin(row_angle)
    for r in range(ROWS // GRID):
        COS[r * GRID : (r + 1) * GRID, :] = jnp.where(by_row, row_cos[r : r + 1, :], column_cos)
        sine = jnp.where(by_row, row_sin[r : r + 1, :], column_sin)
        SIN[r * GRID : (r + 1) * GRID, :] = jnp.where(negative, -sine, sine)

    negative = (lax.broadcasted_iota(jnp.int32, (256, HEAD), 1) // 32) % 2 == 0
    row256 = lax.broadcasted_iota(jnp.int32, (256, 1), 0)

    def rotate(u, cosine, sine):
        turned = jnp.where(negative, pltpu.roll(u, 96, 1), pltpu.roll(u, 32, 1))
        return (u * cosine + turned * sine).astype(BF16)

    def weight(ref, c0):
        return ref[:, :, :, c0 : c0 + 256].reshape(WIDTH, 256)

    def project(m):
        rows = slice(256 * m, 256 * m + 256)
        blocks = ORDER[2 * m : 2 * m + 2]
        cosine = jnp.concatenate([COS[b * 128 : b * 128 + 128, :] for b in blocks], 0)
        sine = jnp.concatenate([SIN[b * 128 : b * 128 + 128, :] for b in blocks], 0)
        q = jnp.dot(T[rows, :], weight(WA, 0), preferred_element_type=F32)
        for h in range(2):
            u = rotate(q[:, h * HEAD : (h + 1) * HEAD], cosine, sine)
            for i, b in enumerate(blocks):
                Q[b, h * 128 : (h + 1) * 128, :] = u[i * 128 : (i + 1) * 128]
        kv = jnp.dot(T[rows, :], weight(WA, 256), preferred_element_type=F32)
        k = rotate(kv[:, :HEAD], cosine, sine)
        v = kv[:, HEAD:].astype(BF16)
        for i, b in enumerate(blocks):
            KV[b + 1, :, 0:HEAD] = k[i * 128 : (i + 1) * 128]
            KV[b + 1, :, HEAD:] = v[i * 128 : (i + 1) * 128]

    def project_conv(m):
        rows = slice(256 * m, 256 * m + 256)
        blocks = ORDER[2 * m : 2 * m + 2]
        c_in = jnp.dot(T[rows, :], weight(WB, 0), preferred_element_type=F32)
        before = jnp.dot(T[rows, :], weight(WB, 256), preferred_element_type=F32)
        sec = (before * c_in).astype(BF16)
        for i, b in enumerate(blocks):
            SEC[b] = sec[i * 128 : (i + 1) * 128].astype(F32)
            if m == 0:
                ES[i] = sec[0:16] if i == 0 else sec[240:256]
        after = jnp.dot(T[rows, :], weight(WD, 0), preferred_element_type=F32)
        for i, b in enumerate(blocks):
            GA[b] = after[i * 128 : (i + 1) * 128]

    row128 = lax.broadcasted_iota(jnp.int32, (128, 1), 0)
    taps = taps_v[...].astype(F32)

    def convolve(b):
        sec = SEC[b]
        if b > 0:
            low = SEC[b - 1, 127:128, :]
        else:
            low = jnp.where(s > 0, ER[0].astype(F32)[15:16, :], 0.0)
        if b < 5:
            high = SEC[b + 1, 0:1, :]
        else:
            high = jnp.where(s < NSP - 1, ER[1].astype(F32)[0:1, :], 0.0)
        before = jnp.where(row128 == 0, low, pltpu.roll(sec, 1, 0))
        later = jnp.where(row128 == 127, high, pltpu.roll(sec, 127, 0))
        mix = before * taps[0:1] + sec * taps[1:2] + later * taps[2:3]
        MC[x, b * 128 : (b + 1) * 128, :] = (GA[b] * mix).astype(BF16)

    qi = lax.broadcasted_iota(jnp.int32, (256, 384), 0) % 128
    kj = lax.broadcasted_iota(jnp.int32, (256, 384), 1)
    inside = (kj >= qi) & (kj <= qi + 256)
    sink_col = jnp.where(row256 < 128, sink[0], sink[1])

    def attend(b):
        keys = KV[b : b + 3, :, 0:HEAD].reshape(384, HEAD)
        values = KV[b : b + 3, :, HEAD:].reshape(384, HEAD)
        scores = nt_dot(Q[b], keys) * HEAD ** (-0.5)
        valid = inside
        if b == 0:
            valid = valid & ((kj >= 128) | (s > 0))
        if b == 5:
            valid = valid & ((kj < 256) | (s < NSP - 1))
        scores = jnp.where(valid, scores, NEG_BIG)
        top = jnp.maximum(jnp.max(scores, 1, keepdims=True), sink_col)
        w = jnp.exp(scores - top)
        total = jnp.sum(w, 1, keepdims=True) + jnp.exp(sink_col - top)
        probs = (w / total).astype(BF16)
        o = jnp.dot(probs, values, preferred_element_type=F32).astype(BF16)
        rows = slice(b * 128, b * 128 + 128)
        MA[x, rows, 0:HEAD] = o[:128]
        MA[x, rows, HEAD : 2 * HEAD] = o[128:]

    def halo_send():
        send(KV.at[1], KV.at[7], hrec.at[0], sm, csem.at[5])
        send(KV.at[6], KV.at[0], hrec.at[1], sp, csem.at[5])

    def edge_send():
        send(ES.at[0], ER.at[1], hrec.at[2], sm, csem.at[6])
        send(ES.at[1], ER.at[0], hrec.at[3], sp, csem.at[6])

    def halo_left():
        arrived(KV.at[0], hrec.at[1])

    def edge_left():
        arrived(ER.at[0], hrec.at[3])

    def halo_right():
        arrived(KV.at[7], hrec.at[0])
        arrived(ER.at[1], hrec.at[2])

    M = (MA, MC)

    def mix(h, d, r0, n):
        return M[h].at[(x + d) % NX, pl.ds(r0, n)]

    def mix_send(h, g):
        blk = mix(h, 0, 256 * g, 256)
        send(blk, blk, mixrec.at[2 * g + h, 0], xp, csem.at[7])
        send(blk, blk, mixrec.at[2 * g + h, 1], xm, csem.at[7])

    def mix_relay(h, g):
        arrived(mix(h, 3, 256 * g, 256), mixrec.at[2 * g + h, 0])
        blk = mix(h, 3, 256 * g, 128)
        send(blk, blk, mixrec.at[2 * g + h, 2], xp, csem.at[7])
        arrived(mix(h, 1, 256 * g, 256), mixrec.at[2 * g + h, 1])
        blk = mix(h, 1, 256 * g + 128, 128)
        send(blk, blk, mixrec.at[2 * g + h, 3], xm, csem.at[7])

    def partial(g, d):
        o = (x + d) % NX
        rows = slice(256 * g, 256 * g + 256)
        return sum(
            nt_dot(M[h][o, rows, :], WO[h][:, :, pl.ds(o, 1)].reshape(QUARTER, 256)) for h in range(2)
        )

    def final_near(g):
        PX[g] = partial(g, 0) + partial(g, 1) + partial(g, 3)

    def final_far(g):
        for h in range(2):
            arrived(mix(h, 2, 256 * g, 128), mixrec.at[2 * g + h, 2])
            arrived(mix(h, 2, 256 * g + 128, 128), mixrec.at[2 * g + h, 3])
        PX[g] += partial(g, 2)
        for half in range(2):
            rows = slice(128 * half, 128 * half + 128)
            t = PX[g, rows, :]
            mean = jnp.sum(t, 1, keepdims=True) * (1.0 / QUARTER)
            m2 = jnp.sum(jnp.square(t - mean), 1, keepdims=True)
            lane = lax.broadcasted_iota(jnp.int32, (128, 128), 1)
            both = jnp.where(lane == 0, mean, m2)
            ST[g, 0, half] = jnp.transpose(both)[0:8, :]
        for d, peer, slot in ((1, xp, 3), (3, xm, 1), (2, x2, 2)):
            send(ST.at[g, 0], ST.at[g, slot], strec.at[g], peer, csem.at[9])

    def finish(g):
        arrived(ST.at[g, pl.ds(1, 3)], strec.at[g])
        for half in range(2):
            rows = slice(128 * half, 128 * half + 128)
            parts = [ST[g, slot, half] for slot in range(4)]
            means = [p[0:1, :] for p in parts]
            mean = (means[0] + means[1] + means[2] + means[3]) * 0.25
            m2 = sum(p[1:2, :] for p in parts)
            for m in means:
                m2 = m2 + QUARTER * jnp.square(m - mean)
            scale = lax.rsqrt(m2 * (1.0 / WIDTH) + EPS)
            line = lax.broadcasted_iota(jnp.int32, (128, 128), 0)
            columns = jnp.transpose(jnp.where(line == 0, mean, scale))
            normed = (PX[g, rows, :] - columns[:, 0:1]) * columns[:, 1:2] * gain_v[0:1, :]
            out[256 * g + 128 * half : 256 * g + 128 * half + 128, :] = normed.astype(BF16)

    outs = []
    on_core(
        0,
        (a_ysend, 0), (a_zsend, 0), (a_y, 0), (a_hop, 0, 1),
        (x_relay, 0), (wo_x,), (x_relay, 1), (x_send, 3),
        (a_hop, 0, 2), (x_relay, 2), (a_hop, 0, 3), (wo_slot, 0, 0), (a_hop, 0, 4), (x_relay, 3),
    )
    on_core(
        1,
        (b_start, 1), (b_zy, 1, 0), (b_start, 3),
        (b_z, 1, 1), (b_zy, 1, 1), (b_zy, 3, 0), (b_z, 3, 1), (b_zy, 3, 1),
        (b_z, 1, 2), (b_zy, 1, 2), (b_y, 1, 0), (b_z, 3, 2), (b_zy, 3, 2), (b_y, 3, 0), (b_y, 1, 1),
        (x_relay, 0), (wo_x,), (x_relay, 1), (x_send, 3),
        (b_z, 1, 3), (b_zy, 1, 3), (b_y, 3, 1), (b_z, 3, 3), (b_zy, 3, 3),
        (b_d, 1, 0), (b_d, 3, 0), (b_y, 1, 2), (b_d, 1, 1), (b_y, 3, 2),
        (b_z, 1, 4), (b_zy, 1, 4), (b_d, 3, 1), (b_z, 3, 4), (b_zy, 3, 4),
        (x_relay, 2), (b_y, 1, 3), (b_y, 3, 3), (wo_slot, 1, 0), (b_d, 1, 2), (b_d, 3, 2), (b_y, 1, 4), (b_y, 3, 4),
        (x_relay, 3), (b_d, 1, 3), (b_d, 3, 3), (all_from_sib, 0),
    )
    x_rest(0)
    x_rest(1)
    project(0)
    halo_send()
    on_core(0, (wo_slot, 0, 1))
    on_core(1, (b_d, 1, 4), (b_d, 3, 4), (wo_slot, 1, 1))
    x_rest(2)
    project(1)
    attend(1)
    halo_left()
    attend(0)
    mix_send(0, 0)
    on_core(0, (all_from_sib, 1), (all_from_sib, 3))
    project_conv(0)
    edge_send()
    project_conv(1)
    convolve(1)
    edge_left()
    convolve(0)
    mix_send(1, 0)
    on_core(0, (wo_slot, 0, 2))
    on_core(1, (wo_slot, 1, 2))
    x_rest(3)
    project(2)
    attend(2)
    attend(3)
    mix_send(0, 1)
    mix_relay(0, 0)
    project_conv(2)
    convolve(2)
    convolve(3)
    mix_send(1, 1)
    on_core(0, (wo_slot, 0, 3))
    on_core(1, (wo_slot, 1, 3))
    mix_relay(1, 0)
    attend(4)
    halo_right()
    attend(5)
    mix_send(0, 2)
    convolve(4)
    convolve(5)
    mix_send(1, 2)
    on_core(0, (wo_slot, 0, 4))
    on_core(1, (wo_slot, 1, 4))
    mix_relay(0, 1)
    on_core(0, (wo_y, 0))
    on_core(1, (wo_y, 1))
    mix_relay(1, 1)
    on_core(0, (wo_d, 0), (wo_end, 0))
    on_core(1, (wo_d, 1), (wo_end, 1))
    mix_relay(0, 2)
    mix_relay(1, 2)
    final_near(0)
    final_far(0)
    final_near(1)
    final_far(1)
    final_near(2)
    final_far(2)
    finish(0)
    finish(1)
    finish(2)
    wo_x_sent()
    wo_sent()
    assert set(counts.values()) == {62}
    for n, w in W.items():
        sent(w.at[z, y, own_rows], csem.at[ICS[n]])

        @pl.when(core == n % 2)
        def _(n=n, w=w):
            sent(w, wsem.at[n // 2, 0])
            sent(w.at[pl.ds(0, 7)], wsem.at[n // 2, 1])
            sent(w.at[0, pl.ds(0, 2)], wsem.at[n // 2, 2])
    sent(T.at[pl.ds(0, 576)], csem.at[4])
    sent(KV.at[pl.ds(0, 2)], csem.at[5])
    sent(ES, csem.at[6])
    sent(T.at[pl.ds(0, 576)], csem.at[7])
    sent(ST.at[:, pl.ds(0, 3)], csem.at[9])


def body(
    tokens, query_weight, key_projection, value_projection, conv_in_weight, conv_gate_out,
    conv_gate_in, conv_taps, head_sink_logit, out_attn_weight, out_conv_weight, out_gain,
):
    half = HEAD // 2
    inverse = np.float32(THETA) ** (-np.arange(0, half, 2, dtype=np.float32) / np.float32(half))
    freq = jnp.asarray(np.tile(inverse.astype(np.float32), 4)[None, :])
    anywhere = pl.BlockSpec(memory_space=pl.ANY)
    specs = [anywhere] * 13
    dma = pltpu.SemaphoreType.DMA
    call = pl.pallas_call(
        kernel,
        out_shape=jax.ShapeDtypeStruct((ROWS, QUARTER), BF16),
        in_specs=specs,
        out_specs=pl.BlockSpec(memory_space=pltpu.VMEM),
        scratch_shapes=[
            pltpu.VMEM((ROWS, WIDTH), BF16),
            pltpu.VMEM((NZ, NY, 64, 512), BF16),
            pltpu.VMEM((NZ, NY, 64, 512), BF16),
            pltpu.VMEM((NZ, NY, 64, 256), BF16),
            pltpu.VMEM((2, NY, NX, 64, 256), BF16),
            pltpu.VMEM((2, NY, NX, 64, 256), BF16),
            pltpu.VMEM((2, 32, 256), BF16),
            pltpu.VMEM((8, 128, 256), BF16),
            pltpu.VMEM((6, 256, 128), BF16),
            pltpu.VMEM((6, 128, 256), F32),
            pltpu.VMEM((6, 128, 256), F32),
            pltpu.VMEM((NX, ROWS, 256), BF16),
            pltpu.VMEM((NX, ROWS, 256), BF16),
            pltpu.VMEM((2, 16, 256), BF16),
            pltpu.VMEM((2, 16, 256), BF16),
            pltpu.VMEM((ROWS, HEAD), F32),
            pltpu.VMEM((ROWS, HEAD), F32),
            pltpu.VMEM((3, 256, QUARTER), F32),
            pltpu.VMEM((3, 4, 2, 8, 128), F32),
            pltpu.VMEM((3, 256), BF16),
            pltpu.VMEM((1, QUARTER), F32),
            pltpu.VMEM((1, HEAD), F32),
            pltpu.SMEM((2,), F32),
            dma((16,)),
            pltpu.SemaphoreType.REGULAR,
            dma((10,)),
            dma((2, 3)),
            dma((2, 32)),
            dma((2, 2)),
            dma((4,)),
            dma((14,)),
            dma((4,)),
            dma((6, 4)),
            dma((3,)),
            dma((1,)),
            dma((4,)),
            dma((2,)),
            dma((3,)),
            dma((3, 2)),
            dma((3,)),
            dma((1,)),
        ],
        compiler_params=pltpu.CompilerParams(
            collective_id=0, has_side_effects=True, vmem_limit_bytes=40 * 1024 * 1024
        ),
    )
    operands = [
        tokens, query_weight, key_projection, value_projection, conv_in_weight, conv_gate_out,
        conv_gate_in, conv_taps, head_sink_logit, out_attn_weight.T, out_conv_weight.T,
        out_gain.reshape(1, -1), freq,
    ]
    return call(*[
        pltpu.with_memory_space_constraint(a, pltpu.HBM) for a in operands
    ])


def solution(mesh):
    return jax.shard_map(
        body,
        mesh=mesh,
        in_specs=(
            P("sp", "tp"),
            P("sp", "tp"),
            P("sp", "tp"),
            P("sp", "tp"),
            P("sp", "tp"),
            P("sp", "tp"),
            P("sp", "tp"),
            P(None, "tp"),
            P("tp"),
            P("tp", "sp"),
            P("tp", "sp"),
            P("tp"),
        ),
        out_specs=P("sp", "tp"),
        check_vma=False,
    )
```

```python
import functools

import jax
import jax.numpy as jnp
import numpy as np
from jax import lax
from jax.experimental import pallas as pl
from jax.experimental.pallas import tpu as pltpu
from jax.sharding import PartitionSpec as P

MESH = pl.DeviceIdType.MESH
F32 = jnp.float32
BF16 = jnp.bfloat16

HEAD = 128
WINDOW = 128
GRID = 64
NEG_BIG = -1e30
THETA = 10000.0
EPS = 1e-05

NZ, NY, NX, NSP = 8, 4, 4, 64
ROWS = 768
WIDTH = 2048
QUARTER = 512
PLACED = (1, 2, 3, 4, 0, 5)
ICS = {0: 1, 1: 3, 3: 8}


def nt_dot(a, b):
    return lax.dot_general(a, b, (((1,), (1,)), ((), ())), preferred_element_type=F32)


def kernel(
    tok, qw, kw, vw, cin, cgo, cgi, taps_in, sink_in, owa, owc, gain_in, freq_in, out,
    T, WA, WB, WD, WOA, WOC, OWN, KV, Q, SEC, GA, MA, MC, ES, ER, COS, SIN, PX, ST,
    taps_v, gain_v, freq_v, sink,
    lsem, met, csem, wsem, wrec, srec, irec, xrec, hrec, mixrec, strec, osem, worec, wozrec, wozsem, woyrec, wosend, wosib,
):
    s = lax.axis_index("sp")
    x = lax.axis_index("tp")
    core = s % 2
    chip = s // 2
    y = chip % NY
    z = chip // NY

    def at(zz, yy, cc):
        return ((zz % NZ) * NY + yy % NY) * 2 + cc

    sib = (at(z, y, 1 - core), x)
    yp, ym, y2 = [(at(z, y + d, core), x) for d in (1, 3, 2)]
    zp, zm = [(at(z + d, y, core), x) for d in (1, NZ - 1)]
    xp, xm, x2 = [(s, (x + d) % NX) for d in (1, 3, 2)]
    sp, sm = [((s + d) % NSP, x) for d in (1, NSP - 1)]

    loads = []

    def load(src, dst):
        cp = pltpu.make_async_copy(src, dst, lsem.at[len(loads)])
        cp.start()
        loads.append(cp)
        return cp

    own_cols = pl.ds(pl.multiple_of(x * QUARTER, QUARTER), QUARTER)
    own_rows = pl.ds(pl.multiple_of(core * 32, 32), 32)
    l_w = [
        load(qw, WA.at[z, y, own_rows, pl.ds(0, 256)]),
        load(kw, WA.at[z, y, own_rows, pl.ds(256, 128)]),
        load(vw, WA.at[z, y, own_rows, pl.ds(384, 128)]),
        load(cin, WB.at[z, y, own_rows, pl.ds(0, 256)]),
        load(cgi, WB.at[z, y, own_rows, pl.ds(256, 256)]),
        load(cgo, WD.at[z, y, own_rows]),
        load(owa, OWN.at[0]),
        load(owc, OWN.at[1]),
    ]
    l_t = [
        load(tok.at[pl.ds(256 * m, 256), :], T.at[pl.ds(256 * m, 256), own_cols]) for m in range(3)
    ]
    l_small = [load(taps_in, taps_v), load(gain_in, gain_v), load(freq_in, freq_v), load(sink_in, sink)]

    barrier = pltpu.get_barrier_semaphore()

    def greet(peer):
        pl.semaphore_signal(barrier, inc=1, device_id=peer, device_id_type=MESH)

    greet(sib)
    for d in (1, 3):
        greet((at(z, y, 0), (x + d) % NX))
        greet((at(z, y + d, 1), x))
    for d in (1, NZ - 1):
        greet((at(z + d, y, 1), x))

    @pl.when(core == 0)
    def _():
        greet((at(z, y + 2, 1), x))

    for cp in l_w:
        cp.wait()

    @pl.when(core == 0)
    def _():
        pl.semaphore_wait(barrier, 5)
        pl.semaphore_signal(met, inc=1, device_id=sib, device_id_type=MESH)

    @pl.when(core == 1)
    def _():
        pl.semaphore_wait(met, 1)

    counts = {0: 0, 1: 0, 3: 0}

    def copy(src, dst, rsem, peer, ssem):
        return pltpu.make_async_remote_copy(
            src_ref=src, dst_ref=dst, send_sem=ssem, recv_sem=rsem,
            device_id=peer, device_id_type=MESH,
        )

    def send(src, dst, rsem, peer, ssem):
        copy(src, dst, rsem, peer, ssem).start()

    def send_weights(n, src, rsem, peer):
        i = counts[n]
        counts[n] += 1
        send(src, src, rsem, peer, wsem.at[n // 2, 0 if i < 32 else 1 if i < 60 else 2])

    def sent(ref, ssem):
        copy(ref, ref, osem.at[0], xp, ssem).wait_send()

    def on_core(c, *steps):
        @pl.when(core == c)
        def _():
            for step, *args in steps:
                step(*args)

    def arrived(ref, rsem):
        copy(ref, ref, rsem, xp, csem.at[0]).wait_recv()

    sib_rows = pl.ds(pl.multiple_of((1 - core) * 32, 32), 32)
    W = {0: WA, 1: WB, 3: WD}
    for n, w in W.items():
        send(w.at[z, y, own_rows], w.at[z, y, own_rows], irec.at[n], sib, csem.at[ICS[n]])

    def from_sib(n):
        arrived(W[n].at[z, y, sib_rows], irec.at[n])

    def cols(d):
        return pl.ds(pl.multiple_of(((x + d) % NX) * QUARTER, QUARTER), QUARTER)

    def t_block(b, d):
        return T.at[pl.ds(128 * b, 128), cols(d)]

    def x_send(m):
        for b in (2 * m, 2 * m + 1):
            send(t_block(b, 0), t_block(b, 0), xrec.at[0, b], xp, csem.at[4])
        for b in (2 * m + 1, 2 * m):
            send(t_block(b, 0), t_block(b, 0), xrec.at[1, b], xm, csem.at[4])

    def x_relay(m):
        b = 2 * m
        arrived(t_block(b, 3), xrec.at[0, b])
        send(t_block(b, 3), t_block(b, 3), xrec.at[2, b], xp, csem.at[4])
        b = 2 * m + 1
        arrived(t_block(b, 1), xrec.at[1, b])
        send(t_block(b, 1), t_block(b, 1), xrec.at[2, b], xm, csem.at[4])

    def x_rest(m):
        arrived(t_block(2 * m, 1), xrec.at[1, 2 * m])
        arrived(t_block(2 * m + 1, 3), xrec.at[0, 2 * m + 1])
        for b in (2 * m, 2 * m + 1):
            arrived(t_block(b, 2), xrec.at[2, b])

    for m in range(2):
        l_t[m].wait()
        x_send(m)
    l_t[2].wait()

    @pl.when(core == 1)
    def _():
        pl.semaphore_wait(barrier, 10)
        pl.semaphore_signal(met, inc=1, device_id=sib, device_id_type=MESH)

    @pl.when(core == 0)
    def _():
        pl.semaphore_wait(met, 1)

    def rel(dz, dy):
        return (dz % NZ) * NY + dy % NY

    def piece(n, dz, dy):
        return W[n].at[(z + dz) % NZ, (y + dy) % NY]

    def fwd(n, dz, dy, peer, ddz, ddy):
        p = piece(n, dz, dy)
        send_weights(n, p, wrec.at[n // 2, rel(dz + ddz, dy + ddy)], peer)

    def to_sib(n, dz, dy):
        p = piece(n, dz, dy)
        send_weights(n, p, srec.at[n // 2, 1 if dz == 0 else 0], sib)

    def got(n, dz, dy):
        arrived(piece(n, dz, dy), wrec.at[n // 2, rel(dz, dy)])

    def all_from_sib(n):
        from_sib(n)
        arrived(W[n].at[pl.ds(0, 7)], srec.at[n // 2, 0])
        arrived(W[n].at[0, pl.ds(0, 3)], srec.at[n // 2, 1])

    def a_ysend(n):
        from_sib(n)
        fwd(n, 0, 0, yp, 0, -1)
        fwd(n, 0, 0, ym, 0, 1)
        fwd(n, 0, 0, y2, 0, 2)

    def a_zsend(n):
        fwd(n, 0, 0, zp, -1, 0)
        fwd(n, 0, 0, zm, 1, 0)

    def a_y(n):
        for dy in (1, 3, 2):
            got(n, 0, dy)
            fwd(n, 0, dy, zp, -1, 0)
            fwd(n, 0, dy, zm, 1, 0)
            to_sib(n, 0, dy)

    def a_hop(n, k, part=(0, 1, 2, 3)):
        for i in part:
            dy = (0, 1, 3, 2)[i]
            for dz in (-k, k) if k < 4 else (4,):
                got(n, dz, dy)
                if dz < 0 and (k < 3 or i % 2 == 0):
                    fwd(n, dz, dy, zp, -1, 0)
                if 0 < dz < 4 and (k < 3 or i % 2 == 1):
                    fwd(n, dz, dy, zm, 1, 0)
                to_sib(n, dz, dy)

    def ring(k):
        return (0,) if k == 0 else (-k, k) if k < 4 else (4,)

    def b_start(n):
        from_sib(n)
        fwd(n, 0, 0, zp, -1, 0)
        fwd(n, 0, 0, zm, 1, 0)

    def b_z(n, k):
        for dz in ring(k):
            got(n, dz, 0)
            if dz < 0:
                fwd(n, dz, 0, zp, -1, 0)
            elif k < 3:
                fwd(n, dz, 0, zm, 1, 0)
            to_sib(n, dz, 0)

    def b_zy(n, k):
        for dz in ring(k):
            fwd(n, dz, 0, yp, 0, -1)
            fwd(n, dz, 0, ym, 0, 1)

    def b_y(n, k):
        for dz in ring(k):
            up = k == 0 or 0 < dz < 4
            got(n, dz, 3)
            if up:
                fwd(n, dz, 3, yp, 0, -1)
            to_sib(n, dz, 3)
            got(n, dz, 1)
            if not up:
                fwd(n, dz, 1, ym, 0, 1)
            to_sib(n, dz, 1)

    def b_d(n, k):
        for dz in ring(k):
            got(n, dz, 2)
            to_sib(n, dz, 2)

    WO = (WOA, WOC)
    owner = z // 2
    place = (z + NZ - 2 * x) % NZ
    right = (place >= 1) & (place <= 4)
    dist = jnp.where(right, place - 1, (NZ - place) % NZ)
    u1 = jnp.where(right, 1, 0)
    u2 = 1 - u1
    onward = (at(z + jnp.where(right, 1, NZ - 1), y, core), x)
    back = (at(z + jnp.where(right, NZ - 1, 1), y, core), x)

    def wo_x():
        for h in range(2):
            here = (owner == x) & (core == h)

            @pl.when(here)
            def _(h=h):
                WO[h][z % 2, y, x, own_rows, :] = OWN[h]

            @pl.when(jnp.logical_not(here))
            def _(h=h):
                send(
                    OWN.at[h], WO[h].at[z % 2, y, x, own_rows], worec.at[(x + NX - owner) % NX],
                    (at(z, y, h), owner), csem.at[2 * h],
                )

    def wo_x_sent():
        for h in range(2):
            @pl.when(jnp.logical_not((owner == x) & (core == h)))
            def _(h=h):
                sent(OWN.at[h], csem.at[2 * h])

    def wo_share(h, u):
        unit = WO[h].at[u, y]
        send(unit, unit, woyrec.at[0, u], yp, wosend.at[0])
        send(unit, unit, woyrec.at[1, u], ym, wosend.at[0])
        send(unit, unit, wosib.at[0], sib, wosend.at[2])

    def wo_slot(h, k):
        if k < 4:
            @pl.when(dist == k)
            def _():
                unit = WO[h].at[u1, y]
                if k == 0:
                    arrived(WO[h].at[z % 2, y, x, sib_rows], worec.at[0])
                    for d in (1, 2, 3):
                        arrived(WO[h].at[z % 2, y, (x + d) % NX], worec.at[d])
                    send(unit, unit, wozrec.at[1], back, wozsem.at[1])
                else:
                    arrived(unit, wozrec.at[0])
                if k < 3:
                    send(unit, unit, wozrec.at[0], onward, wozsem.at[0])
                wo_share(h, u1)
        if k > 0:
            @pl.when(dist == k - 1)
            def _():
                unit = WO[h].at[u2, y]
                arrived(unit, wozrec.at[1])
                if k < 4:
                    send(unit, unit, wozrec.at[1], onward, wozsem.at[2])
                wo_share(h, u2)

    def wo_y(h):
        for u in range(2):
            for d, o in ((3, 0), (1, 1)):
                unit = WO[h].at[u, (y + d) % NY]
                arrived(unit, woyrec.at[o, u])
                if u == o:
                    send(unit, unit, woyrec.at[2, u], yp if u == 0 else ym, wosend.at[1])
                send(unit, unit, wosib.at[0], sib, wosend.at[2])

    def wo_d(h):
        for u in range(2):
            unit = WO[h].at[u, (y + 2) % NY]
            arrived(unit, woyrec.at[2, u])
            send(unit, unit, wosib.at[0], sib, wosend.at[2])

    def wo_end(h):
        arrived(WO[1 - h], wosib.at[0])

    def wo_sent():
        unit = WOA.at[0, 0]
        sent(WOA.at[0], wosend.at[0])
        sent(WOA.at[0, pl.ds(0, 2)], wosend.at[1])
        sent(WOA, wosend.at[2])

        @pl.when(dist < 3)
        def _():
            sent(unit, wozsem.at[0])

        @pl.when(dist < 4)
        def _():
            @pl.when(dist < 3)
            def _():
                sent(unit, wozsem.at[2])

        @pl.when(dist == 0)
        def _():
            sent(unit, wozsem.at[1])

    for cp in l_small:
        cp.wait()
    lane = lax.broadcasted_iota(jnp.int32, (GRID, HEAD), 1)
    line = lax.broadcasted_iota(jnp.int32, (GRID, HEAD), 0).astype(F32)
    by_row = lane < HEAD // 2
    negative = (lane // 32) % 2 == 0
    freq = freq_v[0:1, :]
    column_angle = line * freq
    column_cos, column_sin = jnp.cos(column_angle), jnp.sin(column_angle)
    first = (s * (ROWS // GRID)).astype(F32)
    row_angle = (lax.broadcasted_iota(jnp.int32, (16, HEAD), 0).astype(F32) + first) * freq
    row_cos, row_sin = jnp.cos(row_angle), jnp.sin(row_angle)
    for r in range(ROWS // GRID):
        COS[r * GRID : (r + 1) * GRID, :] = jnp.where(by_row, row_cos[r : r + 1, :], column_cos)
        sine = jnp.where(by_row, row_sin[r : r + 1, :], column_sin)
        SIN[r * GRID : (r + 1) * GRID, :] = jnp.where(negative, -sine, sine)

    negative = (lax.broadcasted_iota(jnp.int32, (256, HEAD), 1) // 32) % 2 == 0
    row256 = lax.broadcasted_iota(jnp.int32, (256, 1), 0)

    def rotate(u, cosine, sine):
        turned = jnp.where(negative, pltpu.roll(u, 96, 1), pltpu.roll(u, 32, 1))
        return (u * cosine + turned * sine).astype(BF16)

    def weight(ref, c0):
        return ref[:, :, :, c0 : c0 + 256].reshape(WIDTH, 256)

    def project(m):
        rows = slice(256 * m, 256 * m + 256)
        blocks = (2 * m, 2 * m + 1)
        cosine, sine = COS[rows, :], SIN[rows, :]
        q = jnp.dot(T[rows, :], weight(WA, 0), preferred_element_type=F32)
        for h in range(2):
            u = rotate(q[:, h * HEAD : (h + 1) * HEAD], cosine, sine)
            for i, b in enumerate(blocks):
                Q[b, h * 128 : (h + 1) * 128, :] = u[i * 128 : (i + 1) * 128]
        kv = jnp.dot(T[rows, :], weight(WA, 256), preferred_element_type=F32)
        k = rotate(kv[:, :HEAD], cosine, sine)
        v = kv[:, HEAD:].astype(BF16)
        for i, b in enumerate(blocks):
            KV[b + 1, :, 0:HEAD] = k[i * 128 : (i + 1) * 128]
            KV[b + 1, :, HEAD:] = v[i * 128 : (i + 1) * 128]

    def project_conv(m):
        rows = slice(256 * m, 256 * m + 256)
        blocks = (2 * m, 2 * m + 1)
        c_in = jnp.dot(T[rows, :], weight(WB, 0), preferred_element_type=F32)
        before = jnp.dot(T[rows, :], weight(WB, 256), preferred_element_type=F32)
        sec = (before * c_in).astype(BF16)
        for i, b in enumerate(blocks):
            SEC[b] = sec[i * 128 : (i + 1) * 128].astype(F32)
        if m == 0:
            ES[0] = sec[0:16]
        if m == 2:
            ES[1] = sec[240:256]
        after = jnp.dot(T[rows, :], weight(WD, 0), preferred_element_type=F32)
        for i, b in enumerate(blocks):
            GA[b] = after[i * 128 : (i + 1) * 128]

    row128 = lax.broadcasted_iota(jnp.int32, (128, 1), 0)
    taps = taps_v[...].astype(F32)

    def placed(b):
        p = PLACED.index(b)
        return slice(128 * p, 128 * p + 128)

    def convolve(b):
        sec = SEC[b]
        if b > 0:
            low = SEC[b - 1, 127:128, :]
        else:
            low = jnp.where(s > 0, ER[0].astype(F32)[15:16, :], 0.0)
        if b < 5:
            high = SEC[b + 1, 0:1, :]
        else:
            high = jnp.where(s < NSP - 1, ER[1].astype(F32)[0:1, :], 0.0)
        before = jnp.where(row128 == 0, low, pltpu.roll(sec, 1, 0))
        later = jnp.where(row128 == 127, high, pltpu.roll(sec, 127, 0))
        mix = before * taps[0:1] + sec * taps[1:2] + later * taps[2:3]
        MC[x, placed(b), :] = (GA[b] * mix).astype(BF16)

    qi = lax.broadcasted_iota(jnp.int32, (256, 384), 0) % 128
    kj = lax.broadcasted_iota(jnp.int32, (256, 384), 1)
    inside = (kj >= qi) & (kj <= qi + 256)
    sink_col = jnp.where(row256 < 128, sink[0], sink[1])

    def attend(b):
        keys = KV[b : b + 3, :, 0:HEAD].reshape(384, HEAD)
        values = KV[b : b + 3, :, HEAD:].reshape(384, HEAD)
        scores = nt_dot(Q[b], keys) * HEAD ** (-0.5)
        valid = inside
        if b == 0:
            valid = valid & ((kj >= 128) | (s > 0))
        if b == 5:
            valid = valid & ((kj < 256) | (s < NSP - 1))
        scores = jnp.where(valid, scores, NEG_BIG)
        top = jnp.maximum(jnp.max(scores, 1, keepdims=True), sink_col)
        w = jnp.exp(scores - top)
        total = jnp.sum(w, 1, keepdims=True) + jnp.exp(sink_col - top)
        probs = (w / total).astype(BF16)
        o = jnp.dot(probs, values, preferred_element_type=F32).astype(BF16)
        rows = placed(b)
        MA[x, rows, 0:HEAD] = o[:128]
        MA[x, rows, HEAD : 2 * HEAD] = o[128:]

    def halo_send(side):
        if side == 0:
            send(KV.at[1], KV.at[7], hrec.at[0], sm, csem.at[5])
        else:
            send(KV.at[6], KV.at[0], hrec.at[1], sp, csem.at[5])

    def edge_send(side):
        if side == 0:
            send(ES.at[0], ER.at[1], hrec.at[2], sm, csem.at[6])
        else:
            send(ES.at[1], ER.at[0], hrec.at[3], sp, csem.at[6])

    def halo_wait():
        arrived(KV.at[0], hrec.at[1])
        arrived(KV.at[7], hrec.at[0])

    def edge_wait():
        arrived(ER.at[0], hrec.at[3])
        arrived(ER.at[1], hrec.at[2])

    M = (MA, MC)

    def mix(h, d, r0, n):
        return M[h].at[(x + d) % NX, pl.ds(r0, n)]

    def mix_send(h, g):
        blk = mix(h, 0, 256 * g, 256)
        send(blk, blk, mixrec.at[2 * g + h, 0], xp, csem.at[7])
        send(blk, blk, mixrec.at[2 * g + h, 1], xm, csem.at[7])

    def mix_relay(h, g):
        arrived(mix(h, 3, 256 * g, 256), mixrec.at[2 * g + h, 0])
        blk = mix(h, 3, 256 * g, 128)
        send(blk, blk, mixrec.at[2 * g + h, 2], xp, csem.at[7])
        arrived(mix(h, 1, 256 * g, 256), mixrec.at[2 * g + h, 1])
        blk = mix(h, 1, 256 * g + 128, 128)
        send(blk, blk, mixrec.at[2 * g + h, 3], xm, csem.at[7])

    def partial(g, d):
        o = (x + d) % NX
        rows = slice(256 * g, 256 * g + 256)
        return sum(
            nt_dot(M[h][o, rows, :], WO[h][:, :, pl.ds(o, 1)].reshape(QUARTER, 256)) for h in range(2)
        )

    def final_near(g):
        PX[g] = partial(g, 0) + partial(g, 1) + partial(g, 3)

    def final_far(g):
        for h in range(2):
            arrived(mix(h, 2, 256 * g, 128), mixrec.at[2 * g + h, 2])
            arrived(mix(h, 2, 256 * g + 128, 128), mixrec.at[2 * g + h, 3])
        PX[g] += partial(g, 2)
        for half in range(2):
            rows = slice(128 * half, 128 * half + 128)
            t = PX[g, rows, :]
            mean = jnp.sum(t, 1, keepdims=True) * (1.0 / QUARTER)
            m2 = jnp.sum(jnp.square(t - mean), 1, keepdims=True)
            lane = lax.broadcasted_iota(jnp.int32, (128, 128), 1)
            both = jnp.where(lane == 0, mean, m2)
            ST[g, 0, half] = jnp.transpose(both)[0:8, :]
        for d, peer, slot in ((1, xp, 3), (3, xm, 1), (2, x2, 2)):
            send(ST.at[g, 0], ST.at[g, slot], strec.at[g], peer, csem.at[9])

    def finish(g):
        arrived(ST.at[g, pl.ds(1, 3)], strec.at[g])
        for half in range(2):
            rows = slice(128 * half, 128 * half + 128)
            parts = [ST[g, slot, half] for slot in range(4)]
            means = [p[0:1, :] for p in parts]
            mean = (means[0] + means[1] + means[2] + means[3]) * 0.25
            m2 = sum(p[1:2, :] for p in parts)
            for m in means:
                m2 = m2 + QUARTER * jnp.square(m - mean)
            scale = lax.rsqrt(m2 * (1.0 / WIDTH) + EPS)
            line = lax.broadcasted_iota(jnp.int32, (128, 128), 0)
            columns = jnp.transpose(jnp.where(line == 0, mean, scale))
            normed = (PX[g, rows, :] - columns[:, 0:1]) * columns[:, 1:2] * gain_v[0:1, :]
            out[PLACED[2 * g + half] * 128 : PLACED[2 * g + half] * 128 + 128, :] = normed.astype(BF16)

    outs = []
    on_core(
        0,
        (a_ysend, 0), (a_zsend, 0), (a_y, 0), (a_hop, 0, 1),
        (x_relay, 0), (wo_x,), (x_relay, 1), (x_send, 2),
        (a_hop, 0, 2), (a_hop, 0, 3), (wo_slot, 0, 0), (a_hop, 0, 4),
    )
    on_core(
        1,
        (b_start, 1), (b_zy, 1, 0), (b_start, 3),
        (b_z, 1, 1), (b_zy, 1, 1), (b_zy, 3, 0), (b_z, 3, 1), (b_zy, 3, 1),
        (b_z, 1, 2), (b_zy, 1, 2), (b_y, 1, 0), (b_z, 3, 2), (b_zy, 3, 2), (b_y, 3, 0), (b_y, 1, 1),
        (x_relay, 0), (wo_x,), (x_relay, 1), (x_send, 2),
        (b_z, 1, 3), (b_zy, 1, 3), (b_y, 3, 1), (b_z, 3, 3), (b_zy, 3, 3),
        (b_d, 1, 0), (b_d, 3, 0), (b_y, 1, 2), (b_d, 1, 1), (b_y, 3, 2),
        (b_z, 1, 4), (b_zy, 1, 4), (b_d, 3, 1), (b_z, 3, 4), (b_zy, 3, 4),
        (b_y, 1, 3), (b_y, 3, 3), (wo_slot, 1, 0), (b_d, 1, 2), (b_d, 3, 2), (b_y, 1, 4), (b_y, 3, 4),
        (b_d, 1, 3), (b_d, 3, 3), (all_from_sib, 0),
    )
    x_rest(0)
    project(0)
    halo_send(0)
    on_core(0, (x_relay, 2), (wo_slot, 0, 1))
    on_core(1, (x_relay, 2), (b_d, 1, 4), (b_d, 3, 4), (wo_slot, 1, 1))
    x_rest(1)
    project(1)
    attend(1)
    attend(2)
    mix_send(0, 0)
    on_core(0, (all_from_sib, 1), (all_from_sib, 3))
    project_conv(0)
    edge_send(0)
    project_conv(1)
    convolve(1)
    convolve(2)
    mix_send(1, 0)
    on_core(0, (wo_slot, 0, 2))
    on_core(1, (wo_slot, 1, 2))
    x_rest(2)
    project(2)
    halo_send(1)
    attend(3)
    attend(4)
    mix_send(0, 1)
    mix_relay(0, 0)
    project_conv(2)
    edge_send(1)
    convolve(3)
    convolve(4)
    mix_send(1, 1)
    on_core(0, (wo_slot, 0, 3))
    on_core(1, (wo_slot, 1, 3))
    mix_relay(1, 0)
    halo_wait()
    attend(0)
    attend(5)
    mix_send(0, 2)
    edge_wait()
    convolve(0)
    convolve(5)
    mix_send(1, 2)
    on_core(0, (wo_slot, 0, 4))
    on_core(1, (wo_slot, 1, 4))
    mix_relay(0, 1)
    on_core(0, (wo_y, 0))
    on_core(1, (wo_y, 1))
    mix_relay(1, 1)
    on_core(0, (wo_d, 0), (wo_end, 0))
    on_core(1, (wo_d, 1), (wo_end, 1))
    mix_relay(0, 2)
    mix_relay(1, 2)
    final_near(0)
    final_far(0)
    final_near(1)
    final_far(1)
    final_near(2)
    final_far(2)
    finish(0)
    finish(1)
    finish(2)
    wo_x_sent()
    wo_sent()
    assert set(counts.values()) == {62}
    for n, w in W.items():
        sent(w.at[z, y, own_rows], csem.at[ICS[n]])

        @pl.when(core == n % 2)
        def _(n=n, w=w):
            sent(w, wsem.at[n // 2, 0])
            sent(w.at[pl.ds(0, 7)], wsem.at[n // 2, 1])
            sent(w.at[0, pl.ds(0, 2)], wsem.at[n // 2, 2])
    sent(T.at[pl.ds(0, 576)], csem.at[4])
    sent(KV.at[pl.ds(0, 2)], csem.at[5])
    sent(ES, csem.at[6])
    sent(T.at[pl.ds(0, 576)], csem.at[7])
    sent(ST.at[:, pl.ds(0, 3)], csem.at[9])


def body(
    tokens, query_weight, key_projection, value_projection, conv_in_weight, conv_gate_out,
    conv_gate_in, conv_taps, head_sink_logit, out_attn_weight, out_conv_weight, out_gain,
):
    half = HEAD // 2
    inverse = np.float32(THETA) ** (-np.arange(0, half, 2, dtype=np.float32) / np.float32(half))
    freq = jnp.asarray(np.tile(inverse.astype(np.float32), 4)[None, :])
    anywhere = pl.BlockSpec(memory_space=pl.ANY)
    specs = [anywhere] * 13
    dma = pltpu.SemaphoreType.DMA
    call = pl.pallas_call(
        kernel,
        out_shape=jax.ShapeDtypeStruct((ROWS, QUARTER), BF16),
        in_specs=specs,
        out_specs=pl.BlockSpec(memory_space=pltpu.VMEM),
        scratch_shapes=[
            pltpu.VMEM((ROWS, WIDTH), BF16),
            pltpu.VMEM((NZ, NY, 64, 512), BF16),
            pltpu.VMEM((NZ, NY, 64, 512), BF16),
            pltpu.VMEM((NZ, NY, 64, 256), BF16),
            pltpu.VMEM((2, NY, NX, 64, 256), BF16),
            pltpu.VMEM((2, NY, NX, 64, 256), BF16),
            pltpu.VMEM((2, 32, 256), BF16),
            pltpu.VMEM((8, 128, 256), BF16),
            pltpu.VMEM((6, 256, 128), BF16),
            pltpu.VMEM((6, 128, 256), F32),
            pltpu.VMEM((6, 128, 256), F32),
            pltpu.VMEM((NX, ROWS, 256), BF16),
            pltpu.VMEM((NX, ROWS, 256), BF16),
            pltpu.VMEM((2, 16, 256), BF16),
            pltpu.VMEM((2, 16, 256), BF16),
            pltpu.VMEM((ROWS, HEAD), F32),
            pltpu.VMEM((ROWS, HEAD), F32),
            pltpu.VMEM((3, 256, QUARTER), F32),
            pltpu.VMEM((3, 4, 2, 8, 128), F32),
            pltpu.VMEM((3, 256), BF16),
            pltpu.VMEM((1, QUARTER), F32),
            pltpu.VMEM((1, HEAD), F32),
            pltpu.SMEM((2,), F32),
            dma((16,)),
            pltpu.SemaphoreType.REGULAR,
            dma((10,)),
            dma((2, 3)),
            dma((2, 32)),
            dma((2, 2)),
            dma((4,)),
            dma((3, 6)),
            dma((4,)),
            dma((6, 4)),
            dma((3,)),
            dma((1,)),
            dma((4,)),
            dma((2,)),
            dma((3,)),
            dma((3, 2)),
            dma((3,)),
            dma((1,)),
        ],
        compiler_params=pltpu.CompilerParams(
            collective_id=0, has_side_effects=True, vmem_limit_bytes=40 * 1024 * 1024
        ),
    )
    operands = [
        tokens, query_weight, key_projection, value_projection, conv_in_weight, conv_gate_out,
        conv_gate_in, conv_taps, head_sink_logit, out_attn_weight.T, out_conv_weight.T,
        out_gain.reshape(1, -1), freq,
    ]
    return call(*[
        pltpu.with_memory_space_constraint(a, pltpu.HBM) for a in operands
    ])


def solution(mesh):
    return jax.shard_map(
        body,
        mesh=mesh,
        in_specs=(
            P("sp", "tp"),
            P("sp", "tp"),
            P("sp", "tp"),
            P("sp", "tp"),
            P("sp", "tp"),
            P("sp", "tp"),
            P("sp", "tp"),
            P(None, "tp"),
            P("tp"),
            P("tp", "sp"),
            P("tp", "sp"),
            P("tp"),
        ),
        out_specs=P("sp", "tp"),
        check_vma=False,
    )
```

```python
import functools

import jax
import jax.numpy as jnp
import numpy as np
from jax import lax
from jax.experimental import pallas as pl
from jax.experimental.pallas import tpu as pltpu
from jax.sharding import PartitionSpec as P

MESH = pl.DeviceIdType.MESH
F32 = jnp.float32
BF16 = jnp.bfloat16

HEAD = 128
WINDOW = 128
GRID = 64
NEG_BIG = -1e30
THETA = 10000.0
EPS = 1e-05

NZ, NY, NX, NSP = 8, 4, 4, 64
ROWS = 768
WIDTH = 2048
QUARTER = 512
PLACED = (1, 2, 3, 4, 0, 5)
ICS = {0: 1, 1: 3, 3: 8}


def nt_dot(a, b):
    return lax.dot_general(a, b, (((1,), (1,)), ((), ())), preferred_element_type=F32)


def kernel(
    tok, qw, kw, vw, cin, cgo, cgi, taps_in, sink_in, owa, owc, gain_in, freq_in, out,
    T, WA, WB, WD, WOA, WOC, OWN, KV, Q, SEC, GA, MA, MC, ES, ER, COS, SIN, PX, ST,
    taps_v, gain_v, freq_v, sink,
    lsem, met, csem, wsem, wrec, srec, irec, xrec, hrec, mixrec, strec, osem, worec, wozrec, wozsem, woyrec, wosend, wosib,
):
    s = lax.axis_index("sp")
    x = lax.axis_index("tp")
    core = s % 2
    chip = s // 2
    y = chip % NY
    z = chip // NY

    def at(zz, yy, cc):
        return ((zz % NZ) * NY + yy % NY) * 2 + cc

    sib = (at(z, y, 1 - core), x)
    yp, ym, y2 = [(at(z, y + d, core), x) for d in (1, 3, 2)]
    zp, zm = [(at(z + d, y, core), x) for d in (1, NZ - 1)]
    xp, xm, x2 = [(s, (x + d) % NX) for d in (1, 3, 2)]
    sp, sm = [((s + d) % NSP, x) for d in (1, NSP - 1)]

    loads = []

    def load(src, dst):
        cp = pltpu.make_async_copy(src, dst, lsem.at[len(loads)])
        cp.start()
        loads.append(cp)
        return cp

    own_cols = pl.ds(pl.multiple_of(x * QUARTER, QUARTER), QUARTER)
    own_rows = pl.ds(pl.multiple_of(core * 32, 32), 32)
    l_w = [
        load(qw, WA.at[z, y, own_rows, pl.ds(0, 256)]),
        load(kw, WA.at[z, y, own_rows, pl.ds(256, 128)]),
        load(vw, WA.at[z, y, own_rows, pl.ds(384, 128)]),
        load(cin, WB.at[z, y, own_rows, pl.ds(0, 256)]),
        load(cgi, WB.at[z, y, own_rows, pl.ds(256, 256)]),
        load(cgo, WD.at[z, y, own_rows]),
        load(owa, OWN.at[0]),
        load(owc, OWN.at[1]),
    ]
    l_t = [
        load(tok.at[pl.ds(256 * m, 256), :], T.at[pl.ds(256 * m, 256), own_cols]) for m in range(3)
    ]
    l_small = [load(taps_in, taps_v), load(gain_in, gain_v), load(freq_in, freq_v), load(sink_in, sink)]

    barrier = pltpu.get_barrier_semaphore()

    def greet(peer):
        pl.semaphore_signal(barrier, inc=1, device_id=peer, device_id_type=MESH)

    greet(sib)
    for d in (1, 3):
        greet((at(z, y, 0), (x + d) % NX))
        greet((at(z, y + d, 1), x))
    for d in (1, NZ - 1):
        greet((at(z + d, y, 1), x))

    @pl.when(core == 0)
    def _():
        greet((at(z, y + 2, 1), x))

    for cp in l_w:
        cp.wait()

    @pl.when(core == 0)
    def _():
        pl.semaphore_wait(barrier, 5)
        pl.semaphore_signal(met, inc=1, device_id=sib, device_id_type=MESH)

    @pl.when(core == 1)
    def _():
        pl.semaphore_wait(met, 1)

    counts = {0: 0, 1: 0, 3: 0}

    def copy(src, dst, rsem, peer, ssem):
        return pltpu.make_async_remote_copy(
            src_ref=src, dst_ref=dst, send_sem=ssem, recv_sem=rsem,
            device_id=peer, device_id_type=MESH,
        )

    def send(src, dst, rsem, peer, ssem):
        copy(src, dst, rsem, peer, ssem).start()

    def send_weights(n, src, rsem, peer):
        i = counts[n]
        counts[n] += 1
        send(src, src, rsem, peer, wsem.at[n // 2, 0 if i < 32 else 1 if i < 60 else 2])

    def sent(ref, ssem):
        copy(ref, ref, osem.at[0], xp, ssem).wait_send()

    def on_core(c, *steps):
        @pl.when(core == c)
        def _():
            for step, *args in steps:
                step(*args)

    def arrived(ref, rsem):
        copy(ref, ref, rsem, xp, csem.at[0]).wait_recv()

    sib_rows = pl.ds(pl.multiple_of((1 - core) * 32, 32), 32)
    W = {0: WA, 1: WB, 3: WD}
    for n, w in W.items():
        send(w.at[z, y, own_rows], w.at[z, y, own_rows], irec.at[n], sib, csem.at[ICS[n]])

    def from_sib(n):
        arrived(W[n].at[z, y, sib_rows], irec.at[n])

    def cols(d):
        return pl.ds(pl.multiple_of(((x + d) % NX) * QUARTER, QUARTER), QUARTER)

    def t_block(b, d):
        return T.at[pl.ds(128 * b, 128), cols(d)]

    def x_send(m):
        a, b = t_block(2 * m, 0), t_block(2 * m + 1, 0)
        send(a, a, xrec.at[0, m], xp, csem.at[4])
        send(b, b, xrec.at[2, m], xp, csem.at[4])
        send(b, b, xrec.at[1, m], xm, csem.at[4])
        send(a, a, xrec.at[2, m], xm, csem.at[4])

    def x_relay(m):
        b = 2 * m
        arrived(t_block(b, 3), xrec.at[0, m])
        send(t_block(b, 3), t_block(b, 3), xrec.at[2, m], xp, csem.at[4])
        b = 2 * m + 1
        arrived(t_block(b, 1), xrec.at[1, m])
        send(t_block(b, 1), t_block(b, 1), xrec.at[2, m], xm, csem.at[4])

    def x_rest(m):
        arrived(T.at[pl.ds(0, 128)], xrec.at[2, m])

    for m in range(2):
        l_t[m].wait()
        x_send(m)
    l_t[2].wait()

    @pl.when(core == 1)
    def _():
        pl.semaphore_wait(barrier, 10)
        pl.semaphore_signal(met, inc=1, device_id=sib, device_id_type=MESH)

    @pl.when(core == 0)
    def _():
        pl.semaphore_wait(met, 1)

    def rel(dz, dy):
        return (dz % NZ) * NY + dy % NY

    def piece(n, dz, dy):
        return W[n].at[(z + dz) % NZ, (y + dy) % NY]

    def fwd(n, dz, dy, peer, ddz, ddy):
        p = piece(n, dz, dy)
        send_weights(n, p, wrec.at[n // 2, rel(dz + ddz, dy + ddy)], peer)

    def to_sib(n, dz, dy):
        p = piece(n, dz, dy)
        send_weights(n, p, srec.at[n // 2, 1 if dz == 0 else 0], sib)

    def got(n, dz, dy):
        arrived(piece(n, dz, dy), wrec.at[n // 2, rel(dz, dy)])

    def all_from_sib(n):
        from_sib(n)
        arrived(W[n].at[pl.ds(0, 7)], srec.at[n // 2, 0])
        arrived(W[n].at[0, pl.ds(0, 3)], srec.at[n // 2, 1])

    def a_ysend(n):
        from_sib(n)
        fwd(n, 0, 0, yp, 0, -1)
        fwd(n, 0, 0, ym, 0, 1)
        fwd(n, 0, 0, y2, 0, 2)

    def a_zsend(n):
        fwd(n, 0, 0, zp, -1, 0)
        fwd(n, 0, 0, zm, 1, 0)

    def a_y(n):
        for dy in (1, 3, 2):
            got(n, 0, dy)
            fwd(n, 0, dy, zp, -1, 0)
            fwd(n, 0, dy, zm, 1, 0)
            to_sib(n, 0, dy)

    def a_hop(n, k, part=(0, 1, 2, 3)):
        for i in part:
            dy = (0, 1, 3, 2)[i]
            for dz in (-k, k) if k < 4 else (4,):
                got(n, dz, dy)
                if dz < 0 and (k < 3 or i % 2 == 0):
                    fwd(n, dz, dy, zp, -1, 0)
                if 0 < dz < 4 and (k < 3 or i % 2 == 1):
                    fwd(n, dz, dy, zm, 1, 0)
                to_sib(n, dz, dy)

    def ring(k):
        return (0,) if k == 0 else (-k, k) if k < 4 else (4,)

    def b_start(n):
        from_sib(n)
        fwd(n, 0, 0, zp, -1, 0)
        fwd(n, 0, 0, zm, 1, 0)

    def b_z(n, k):
        for dz in ring(k):
            got(n, dz, 0)
            if dz < 0:
                fwd(n, dz, 0, zp, -1, 0)
            elif k < 3:
                fwd(n, dz, 0, zm, 1, 0)
            to_sib(n, dz, 0)

    def b_zy(n, k):
        for dz in ring(k):
            fwd(n, dz, 0, yp, 0, -1)
            fwd(n, dz, 0, ym, 0, 1)

    def b_y(n, k):
        for dz in ring(k):
            up = k == 0 or 0 < dz < 4
            got(n, dz, 3)
            if up:
                fwd(n, dz, 3, yp, 0, -1)
            to_sib(n, dz, 3)
            got(n, dz, 1)
            if not up:
                fwd(n, dz, 1, ym, 0, 1)
            to_sib(n, dz, 1)

    def b_d(n, k):
        for dz in ring(k):
            got(n, dz, 2)
            to_sib(n, dz, 2)

    WO = (WOA, WOC)
    owner = z // 2
    place = (z + NZ - 2 * x) % NZ
    right = (place >= 1) & (place <= 4)
    dist = jnp.where(right, place - 1, (NZ - place) % NZ)
    u1 = jnp.where(right, 1, 0)
    u2 = 1 - u1
    onward = (at(z + jnp.where(right, 1, NZ - 1), y, core), x)
    back = (at(z + jnp.where(right, NZ - 1, 1), y, core), x)

    def wo_x():
        for h in range(2):
            here = (owner == x) & (core == h)

            @pl.when(here)
            def _(h=h):
                WO[h][z % 2, y, x, own_rows, :] = OWN[h]

            @pl.when(jnp.logical_not(here))
            def _(h=h):
                send(
                    OWN.at[h], WO[h].at[z % 2, y, x, own_rows], worec.at[(x + NX - owner) % NX],
                    (at(z, y, h), owner), csem.at[2 * h],
                )

    def wo_x_sent():
        for h in range(2):
            @pl.when(jnp.logical_not((owner == x) & (core == h)))
            def _(h=h):
                sent(OWN.at[h], csem.at[2 * h])

    def wo_share(h, u):
        unit = WO[h].at[u, y]
        send(unit, unit, woyrec.at[0, u], yp, wosend.at[0])
        send(unit, unit, woyrec.at[1, u], ym, wosend.at[0])
        send(unit, unit, wosib.at[0], sib, wosend.at[2])

    def wo_slot(h, k):
        if k < 4:
            @pl.when(dist == k)
            def _():
                unit = WO[h].at[u1, y]
                if k == 0:
                    arrived(WO[h].at[z % 2, y, x, sib_rows], worec.at[0])
                    for d in (1, 2, 3):
                        arrived(WO[h].at[z % 2, y, (x + d) % NX], worec.at[d])
                    send(unit, unit, wozrec.at[1], back, wozsem.at[1])
                else:
                    arrived(unit, wozrec.at[0])
                if k < 3:
                    send(unit, unit, wozrec.at[0], onward, wozsem.at[0])
                wo_share(h, u1)
        if k > 0:
            @pl.when(dist == k - 1)
            def _():
                unit = WO[h].at[u2, y]
                arrived(unit, wozrec.at[1])
                if k < 4:
                    send(unit, unit, wozrec.at[1], onward, wozsem.at[2])
                wo_share(h, u2)

    def wo_y(h):
        for u in range(2):
            for d, o in ((3, 0), (1, 1)):
                unit = WO[h].at[u, (y + d) % NY]
                arrived(unit, woyrec.at[o, u])
                if u == o:
                    send(unit, unit, woyrec.at[2, u], yp if u == 0 else ym, wosend.at[1])
                send(unit, unit, wosib.at[0], sib, wosend.at[2])

    def wo_d(h):
        for u in range(2):
            unit = WO[h].at[u, (y + 2) % NY]
            arrived(unit, woyrec.at[2, u])
            send(unit, unit, wosib.at[0], sib, wosend.at[2])

    def wo_end(h):
        arrived(WO[1 - h], wosib.at[0])

    def wo_sent():
        unit = WOA.at[0, 0]
        sent(WOA.at[0], wosend.at[0])
        sent(WOA.at[0, pl.ds(0, 2)], wosend.at[1])
        sent(WOA, wosend.at[2])

        @pl.when(dist < 3)
        def _():
            sent(unit, wozsem.at[0])

        @pl.when(dist < 4)
        def _():
            @pl.when(dist < 3)
            def _():
                sent(unit, wozsem.at[2])

        @pl.when(dist == 0)
        def _():
            sent(unit, wozsem.at[1])

    for cp in l_small:
        cp.wait()
    lane = lax.broadcasted_iota(jnp.int32, (GRID, HEAD), 1)
    line = lax.broadcasted_iota(jnp.int32, (GRID, HEAD), 0).astype(F32)
    by_row = lane < HEAD // 2
    negative = (lane // 32) % 2 == 0
    freq = freq_v[0:1, :]
    column_angle = line * freq
    column_cos, column_sin = jnp.cos(column_angle), jnp.sin(column_angle)
    first = (s * (ROWS // GRID)).astype(F32)
    row_angle = (lax.broadcasted_iota(jnp.int32, (16, HEAD), 0).astype(F32) + first) * freq
    row_cos, row_sin = jnp.cos(row_angle), jnp.sin(row_angle)
    for r in range(ROWS // GRID):
        COS[r * GRID : (r + 1) * GRID, :] = jnp.where(by_row, row_cos[r : r + 1, :], column_cos)
        sine = jnp.where(by_row, row_sin[r : r + 1, :], column_sin)
        SIN[r * GRID : (r + 1) * GRID, :] = jnp.where(negative, -sine, sine)

    negative = (lax.broadcasted_iota(jnp.int32, (256, HEAD), 1) // 32) % 2 == 0
    row256 = lax.broadcasted_iota(jnp.int32, (256, 1), 0)

    def rotate(u, cosine, sine):
        turned = jnp.where(negative, pltpu.roll(u, 96, 1), pltpu.roll(u, 32, 1))
        return (u * cosine + turned * sine).astype(BF16)

    def weight(ref, c0):
        return ref[:, :, :, c0 : c0 + 256].reshape(WIDTH, 256)

    def project(m):
        rows = slice(256 * m, 256 * m + 256)
        blocks = (2 * m, 2 * m + 1)
        cosine, sine = COS[rows, :], SIN[rows, :]
        q = jnp.dot(T[rows, :], weight(WA, 0), preferred_element_type=F32)
        for h in range(2):
            u = rotate(q[:, h * HEAD : (h + 1) * HEAD], cosine, sine)
            for i, b in enumerate(blocks):
                Q[b, h * 128 : (h + 1) * 128, :] = u[i * 128 : (i + 1) * 128]
        kv = jnp.dot(T[rows, :], weight(WA, 256), preferred_element_type=F32)
        k = rotate(kv[:, :HEAD], cosine, sine)
        v = kv[:, HEAD:].astype(BF16)
        for i, b in enumerate(blocks):
            KV[b + 1, :, 0:HEAD] = k[i * 128 : (i + 1) * 128]
            KV[b + 1, :, HEAD:] = v[i * 128 : (i + 1) * 128]

    def project_conv(m):
        rows = slice(256 * m, 256 * m + 256)
        blocks = (2 * m, 2 * m + 1)
        c_in = jnp.dot(T[rows, :], weight(WB, 0), preferred_element_type=F32)
        before = jnp.dot(T[rows, :], weight(WB, 256), preferred_element_type=F32)
        sec = (before * c_in).astype(BF16)
        for i, b in enumerate(blocks):
            SEC[b] = sec[i * 128 : (i + 1) * 128].astype(F32)
        if m == 0:
            ES[0] = sec[0:16]
        if m == 2:
            ES[1] = sec[240:256]
        after = jnp.dot(T[rows, :], weight(WD, 0), preferred_element_type=F32)
        for i, b in enumerate(blocks):
            GA[b] = after[i * 128 : (i + 1) * 128]

    row128 = lax.broadcasted_iota(jnp.int32, (128, 1), 0)
    taps = taps_v[...].astype(F32)

    def placed(b):
        p = PLACED.index(b)
        return slice(128 * p, 128 * p + 128)

    def convolve(b):
        sec = SEC[b]
        if b > 0:
            low = SEC[b - 1, 127:128, :]
        else:
            low = jnp.where(s > 0, ER[0].astype(F32)[15:16, :], 0.0)
        if b < 5:
            high = SEC[b + 1, 0:1, :]
        else:
            high = jnp.where(s < NSP - 1, ER[1].astype(F32)[0:1, :], 0.0)
        before = jnp.where(row128 == 0, low, pltpu.roll(sec, 1, 0))
        later = jnp.where(row128 == 127, high, pltpu.roll(sec, 127, 0))
        mix = before * taps[0:1] + sec * taps[1:2] + later * taps[2:3]
        MC[x, placed(b), :] = (GA[b] * mix).astype(BF16)

    qi = lax.broadcasted_iota(jnp.int32, (256, 384), 0) % 128
    kj = lax.broadcasted_iota(jnp.int32, (256, 384), 1)
    inside = (kj >= qi) & (kj <= qi + 256)
    sink_col = jnp.where(row256 < 128, sink[0], sink[1])

    def attend(b):
        keys = KV[b : b + 3, :, 0:HEAD].reshape(384, HEAD)
        values = KV[b : b + 3, :, HEAD:].reshape(384, HEAD)
        scores = nt_dot(Q[b], keys) * HEAD ** (-0.5)
        valid = inside
        if b == 0:
            valid = valid & ((kj >= 128) | (s > 0))
        if b == 5:
            valid = valid & ((kj < 256) | (s < NSP - 1))
        scores = jnp.where(valid, scores, NEG_BIG)
        top = jnp.maximum(jnp.max(scores, 1, keepdims=True), sink_col)
        w = jnp.exp(scores - top)
        total = jnp.sum(w, 1, keepdims=True) + jnp.exp(sink_col - top)
        probs = (w / total).astype(BF16)
        o = jnp.dot(probs, values, preferred_element_type=F32).astype(BF16)
        rows = placed(b)
        MA[x, rows, 0:HEAD] = o[:128]
        MA[x, rows, HEAD : 2 * HEAD] = o[128:]

    def halo_send(side):
        if side == 0:
            send(KV.at[1], KV.at[7], hrec.at[0], sm, csem.at[5])
        else:
            send(KV.at[6], KV.at[0], hrec.at[1], sp, csem.at[5])

    def edge_send(side):
        if side == 0:
            send(ES.at[0], ER.at[1], hrec.at[2], sm, csem.at[6])
        else:
            send(ES.at[1], ER.at[0], hrec.at[3], sp, csem.at[6])

    def halo_wait():
        arrived(KV.at[0], hrec.at[1])
        arrived(KV.at[7], hrec.at[0])

    def edge_wait():
        arrived(ER.at[0], hrec.at[3])
        arrived(ER.at[1], hrec.at[2])

    M = (MA, MC)

    def mix(h, d, r0, n):
        return M[h].at[(x + d) % NX, pl.ds(r0, n)]

    def mix_send(h, g):
        blk = mix(h, 0, 256 * g, 256)
        send(blk, blk, mixrec.at[2 * g + h, 0], xp, csem.at[7])
        send(blk, blk, mixrec.at[2 * g + h, 1], xm, csem.at[7])

    def mix_relay(h, g):
        arrived(mix(h, 3, 256 * g, 256), mixrec.at[2 * g + h, 0])
        blk = mix(h, 3, 256 * g, 128)
        send(blk, blk, mixrec.at[2 * g + h, 2], xp, csem.at[7])
        arrived(mix(h, 1, 256 * g, 256), mixrec.at[2 * g + h, 1])
        blk = mix(h, 1, 256 * g + 128, 128)
        send(blk, blk, mixrec.at[2 * g + h, 2], xm, csem.at[7])

    def partial(g, d):
        o = (x + d) % NX
        rows = slice(256 * g, 256 * g + 256)
        return sum(
            nt_dot(M[h][o, rows, :], WO[h][:, :, pl.ds(o, 1)].reshape(QUARTER, 256)) for h in range(2)
        )

    def final_near(g):
        PX[g] = partial(g, 0) + partial(g, 1) + partial(g, 3)

    def final_far(g):
        for h in range(2):
            arrived(mix(h, 2, 256 * g, 256), mixrec.at[2 * g + h, 2])
        PX[g] += partial(g, 2)
        for half in range(2):
            rows = slice(128 * half, 128 * half + 128)
            t = PX[g, rows, :]
            mean = jnp.sum(t, 1, keepdims=True) * (1.0 / QUARTER)
            m2 = jnp.sum(jnp.square(t - mean), 1, keepdims=True)
            lane = lax.broadcasted_iota(jnp.int32, (128, 128), 1)
            both = jnp.where(lane == 0, mean, m2)
            ST[g, 0, half] = jnp.transpose(both)[0:8, :]
        for d, peer, slot in ((1, xp, 3), (3, xm, 1), (2, x2, 2)):
            send(ST.at[g, 0], ST.at[g, slot], strec.at[g], peer, csem.at[9])

    def finish(g):
        arrived(ST.at[g, pl.ds(1, 3)], strec.at[g])
        for half in range(2):
            rows = slice(128 * half, 128 * half + 128)
            parts = [ST[g, slot, half] for slot in range(4)]
            means = [p[0:1, :] for p in parts]
            mean = (means[0] + means[1] + means[2] + means[3]) * 0.25
            m2 = sum(p[1:2, :] for p in parts)
            for m in means:
                m2 = m2 + QUARTER * jnp.square(m - mean)
            scale = lax.rsqrt(m2 * (1.0 / WIDTH) + EPS)
            line = lax.broadcasted_iota(jnp.int32, (128, 128), 0)
            columns = jnp.transpose(jnp.where(line == 0, mean, scale))
            normed = (PX[g, rows, :] - columns[:, 0:1]) * columns[:, 1:2] * gain_v[0:1, :]
            out[PLACED[2 * g + half] * 128 : PLACED[2 * g + half] * 128 + 128, :] = normed.astype(BF16)

    outs = []
    on_core(
        0,
        (a_ysend, 0), (a_zsend, 0), (a_y, 0), (a_hop, 0, 1),
        (x_relay, 0), (wo_x,), (x_relay, 1), (x_send, 2),
        (a_hop, 0, 2), (a_hop, 0, 3), (wo_slot, 0, 0), (a_hop, 0, 4),
    )
    on_core(
        1,
        (b_start, 1), (b_zy, 1, 0), (b_start, 3),
        (b_z, 1, 1), (b_zy, 1, 1), (b_zy, 3, 0), (b_z, 3, 1), (b_zy, 3, 1),
        (b_z, 1, 2), (b_zy, 1, 2), (b_y, 1, 0), (b_z, 3, 2), (b_zy, 3, 2), (b_y, 3, 0), (b_y, 1, 1),
        (x_relay, 0), (wo_x,), (x_relay, 1), (x_send, 2),
        (b_z, 1, 3), (b_zy, 1, 3), (b_y, 3, 1), (b_z, 3, 3), (b_zy, 3, 3),
        (b_d, 1, 0), (b_d, 3, 0), (b_y, 1, 2), (b_d, 1, 1), (b_y, 3, 2),
        (b_z, 1, 4), (b_zy, 1, 4), (b_d, 3, 1), (b_z, 3, 4), (b_zy, 3, 4),
        (b_y, 1, 3), (b_y, 3, 3), (wo_slot, 1, 0), (b_d, 1, 2), (b_d, 3, 2), (b_y, 1, 4), (b_y, 3, 4),
        (b_d, 1, 3), (b_d, 3, 3), (all_from_sib, 0),
    )
    x_rest(0)
    project(0)
    halo_send(0)
    on_core(0, (x_relay, 2), (wo_slot, 0, 1))
    on_core(1, (x_relay, 2), (b_d, 1, 4), (b_d, 3, 4), (wo_slot, 1, 1))
    x_rest(1)
    project(1)
    attend(1)
    attend(2)
    mix_send(0, 0)
    on_core(0, (all_from_sib, 1), (all_from_sib, 3))
    project_conv(0)
    edge_send(0)
    project_conv(1)
    convolve(1)
    convolve(2)
    mix_send(1, 0)
    on_core(0, (wo_slot, 0, 2))
    on_core(1, (wo_slot, 1, 2))
    x_rest(2)
    project(2)
    halo_send(1)
    attend(3)
    attend(4)
    mix_send(0, 1)
    mix_relay(0, 0)
    project_conv(2)
    edge_send(1)
    convolve(3)
    convolve(4)
    mix_send(1, 1)
    on_core(0, (wo_slot, 0, 3))
    on_core(1, (wo_slot, 1, 3))
    mix_relay(1, 0)
    halo_wait()
    attend(0)
    attend(5)
    mix_send(0, 2)
    edge_wait()
    convolve(0)
    convolve(5)
    mix_send(1, 2)
    on_core(0, (wo_slot, 0, 4))
    on_core(1, (wo_slot, 1, 4))
    mix_relay(0, 1)
    on_core(0, (wo_y, 0))
    on_core(1, (wo_y, 1))
    mix_relay(1, 1)
    on_core(0, (wo_d, 0), (wo_end, 0))
    on_core(1, (wo_d, 1), (wo_end, 1))
    mix_relay(0, 2)
    mix_relay(1, 2)
    wo_x_sent()
    wo_sent()
    assert set(counts.values()) == {62}
    for n, w in W.items():
        sent(w.at[z, y, own_rows], csem.at[ICS[n]])

        @pl.when(core == n % 2)
        def _(n=n, w=w):
            sent(w, wsem.at[n // 2, 0])
            sent(w.at[pl.ds(0, 7)], wsem.at[n // 2, 1])
            sent(w.at[0, pl.ds(0, 2)], wsem.at[n // 2, 2])
    sent(T.at[pl.ds(0, 576)], csem.at[4])
    sent(KV.at[pl.ds(0, 2)], csem.at[5])
    sent(ES, csem.at[6])
    final_near(0)
    final_far(0)
    final_near(1)
    final_far(1)
    final_near(2)
    final_far(2)
    finish(0)
    finish(1)
    finish(2)
    sent(T.at[pl.ds(0, 576)], csem.at[7])
    sent(ST.at[:, pl.ds(0, 3)], csem.at[9])


def body(
    tokens, query_weight, key_projection, value_projection, conv_in_weight, conv_gate_out,
    conv_gate_in, conv_taps, head_sink_logit, out_attn_weight, out_conv_weight, out_gain,
):
    half = HEAD // 2
    inverse = np.float32(THETA) ** (-np.arange(0, half, 2, dtype=np.float32) / np.float32(half))
    freq = jnp.asarray(np.tile(inverse.astype(np.float32), 4)[None, :])
    anywhere = pl.BlockSpec(memory_space=pl.ANY)
    specs = [anywhere] * 13
    dma = pltpu.SemaphoreType.DMA
    call = pl.pallas_call(
        kernel,
        out_shape=jax.ShapeDtypeStruct((ROWS, QUARTER), BF16),
        in_specs=specs,
        out_specs=pl.BlockSpec(memory_space=pltpu.VMEM),
        scratch_shapes=[
            pltpu.VMEM((ROWS, WIDTH), BF16),
            pltpu.VMEM((NZ, NY, 64, 512), BF16),
            pltpu.VMEM((NZ, NY, 64, 512), BF16),
            pltpu.VMEM((NZ, NY, 64, 256), BF16),
            pltpu.VMEM((2, NY, NX, 64, 256), BF16),
            pltpu.VMEM((2, NY, NX, 64, 256), BF16),
            pltpu.VMEM((2, 32, 256), BF16),
            pltpu.VMEM((8, 128, 256), BF16),
            pltpu.VMEM((6, 256, 128), BF16),
            pltpu.VMEM((6, 128, 256), F32),
            pltpu.VMEM((6, 128, 256), F32),
            pltpu.VMEM((NX, ROWS, 256), BF16),
            pltpu.VMEM((NX, ROWS, 256), BF16),
            pltpu.VMEM((2, 16, 256), BF16),
            pltpu.VMEM((2, 16, 256), BF16),
            pltpu.VMEM((ROWS, HEAD), F32),
            pltpu.VMEM((ROWS, HEAD), F32),
            pltpu.VMEM((3, 256, QUARTER), F32),
            pltpu.VMEM((3, 4, 2, 8, 128), F32),
            pltpu.VMEM((3, 256), BF16),
            pltpu.VMEM((1, QUARTER), F32),
            pltpu.VMEM((1, HEAD), F32),
            pltpu.SMEM((2,), F32),
            dma((16,)),
            pltpu.SemaphoreType.REGULAR,
            dma((10,)),
            dma((2, 3)),
            dma((2, 32)),
            dma((2, 2)),
            dma((4,)),
            dma((3, 3)),
            dma((4,)),
            dma((6, 3)),
            dma((3,)),
            dma((1,)),
            dma((4,)),
            dma((2,)),
            dma((3,)),
            dma((3, 2)),
            dma((3,)),
            dma((1,)),
        ],
        compiler_params=pltpu.CompilerParams(
            collective_id=0, has_side_effects=True, vmem_limit_bytes=40 * 1024 * 1024
        ),
    )
    operands = [
        tokens, query_weight, key_projection, value_projection, conv_in_weight, conv_gate_out,
        conv_gate_in, conv_taps, head_sink_logit, out_attn_weight.T, out_conv_weight.T,
        out_gain.reshape(1, -1), freq,
    ]
    return call(*[
        pltpu.with_memory_space_constraint(a, pltpu.HBM) for a in operands
    ])


def solution(mesh):
    return jax.shard_map(
        body,
        mesh=mesh,
        in_specs=(
            P("sp", "tp"),
            P("sp", "tp"),
            P("sp", "tp"),
            P("sp", "tp"),
            P("sp", "tp"),
            P("sp", "tp"),
            P("sp", "tp"),
            P(None, "tp"),
            P("tp"),
            P("tp", "sp"),
            P("tp", "sp"),
            P("tp"),
        ),
        out_specs=P("sp", "tp"),
        check_vma=False,
    )
```

```python
import functools

import jax
import jax.numpy as jnp
import numpy as np
from jax import lax
from jax.experimental import pallas as pl
from jax.experimental.pallas import tpu as pltpu
from jax.sharding import PartitionSpec as P

MESH = pl.DeviceIdType.MESH
F32 = jnp.float32
BF16 = jnp.bfloat16

HEAD = 128
WINDOW = 128
GRID = 64
NEG_BIG = -1e30
THETA = 10000.0
EPS = 1e-05

NZ, NY, NX, NSP = 8, 4, 4, 64
ROWS = 768
WIDTH = 2048
QUARTER = 512
PLACED = (1, 2, 3, 4, 0, 5)
ICS = {0: 1, 1: 3, 3: 8}


def nt_dot(a, b):
    return lax.dot_general(a, b, (((1,), (1,)), ((), ())), preferred_element_type=F32)


def kernel(
    tok, qw, kw, vw, cin, cgo, cgi, taps_in, sink_in, owa, owc, gain_in, freq_in, out,
    T, WA, WB, WD, WOA, WOC, OWN, KV, Q, SEC, GA, MA, MC, ES, ER, COS, SIN, PX, ST,
    taps_v, gain_v, freq_v, sink,
    lsem, met, csem, wsem, wrec, srec, irec, xrec, hrec, mixrec, strec, osem, worec, wozrec, wozsem, woyrec, wosend, wosib,
):
    s = lax.axis_index("sp")
    x = lax.axis_index("tp")
    core = s % 2
    chip = s // 2
    y = chip % NY
    z = chip // NY

    def at(zz, yy, cc):
        return ((zz % NZ) * NY + yy % NY) * 2 + cc

    sib = (at(z, y, 1 - core), x)
    yp, ym, y2 = [(at(z, y + d, core), x) for d in (1, 3, 2)]
    zp, zm = [(at(z + d, y, core), x) for d in (1, NZ - 1)]
    xp, xm, x2 = [(s, (x + d) % NX) for d in (1, 3, 2)]
    sp, sm = [((s + d) % NSP, x) for d in (1, NSP - 1)]

    loads = []

    def load(src, dst):
        cp = pltpu.make_async_copy(src, dst, lsem.at[len(loads)])
        cp.start()
        loads.append(cp)
        return cp

    own_cols = pl.ds(pl.multiple_of(x * QUARTER, QUARTER), QUARTER)
    own_rows = pl.ds(pl.multiple_of(core * 32, 32), 32)
    l_w = [
        load(qw, WA.at[z, y, own_rows, pl.ds(0, 256)]),
        load(kw, WA.at[z, y, own_rows, pl.ds(256, 128)]),
        load(vw, WA.at[z, y, own_rows, pl.ds(384, 128)]),
        load(cin, WB.at[z, y, own_rows, pl.ds(0, 256)]),
        load(cgi, WB.at[z, y, own_rows, pl.ds(256, 256)]),
        load(cgo, WD.at[z, y, own_rows]),
        load(owa, OWN.at[0]),
        load(owc, OWN.at[1]),
    ]
    l_t = [
        load(tok.at[pl.ds(256 * m, 256), :], T.at[pl.ds(256 * m, 256), own_cols]) for m in range(3)
    ]
    l_small = [load(taps_in, taps_v), load(gain_in, gain_v), load(freq_in, freq_v), load(sink_in, sink)]

    barrier = pltpu.get_barrier_semaphore()

    def greet(peer):
        pl.semaphore_signal(barrier, inc=1, device_id=peer, device_id_type=MESH)

    greet(sib)
    for d in (1, 3):
        greet((at(z, y, 0), (x + d) % NX))
        greet((at(z, y + d, 1), x))
    for d in (1, NZ - 1):
        greet((at(z + d, y, 1), x))

    @pl.when(core == 0)
    def _():
        greet((at(z, y + 2, 1), x))

    for cp in l_w:
        cp.wait()

    @pl.when(core == 0)
    def _():
        pl.semaphore_wait(barrier, 5)
        pl.semaphore_signal(met, inc=1, device_id=sib, device_id_type=MESH)

    @pl.when(core == 1)
    def _():
        pl.semaphore_wait(met, 1)

    counts = {0: 0, 1: 0, 3: 0}

    def copy(src, dst, rsem, peer, ssem):
        return pltpu.make_async_remote_copy(
            src_ref=src, dst_ref=dst, send_sem=ssem, recv_sem=rsem,
            device_id=peer, device_id_type=MESH,
        )

    def send(src, dst, rsem, peer, ssem):
        copy(src, dst, rsem, peer, ssem).start()

    def send_weights(n, src, rsem, peer):
        i = counts[n]
        counts[n] += 1
        send(src, src, rsem, peer, wsem.at[n // 2, 0 if i < 32 else 1 if i < 60 else 2])

    def sent(ref, ssem):
        copy(ref, ref, osem.at[0], xp, ssem).wait_send()

    def on_core(c, *steps):
        @pl.when(core == c)
        def _():
            for step, *args in steps:
                step(*args)

    def arrived(ref, rsem):
        copy(ref, ref, rsem, xp, csem.at[0]).wait_recv()

    sib_rows = pl.ds(pl.multiple_of((1 - core) * 32, 32), 32)
    W = {0: WA, 1: WB, 3: WD}
    for n, w in W.items():
        send(w.at[z, y, own_rows], w.at[z, y, own_rows], irec.at[n], sib, csem.at[ICS[n]])

    def from_sib(n):
        arrived(W[n].at[z, y, sib_rows], irec.at[n])

    def cols(d):
        return pl.ds(pl.multiple_of(((x + d) % NX) * QUARTER, QUARTER), QUARTER)

    def t_block(b, d):
        return T.at[pl.ds(128 * b, 128), cols(d)]

    def x_send(m):
        a, b = t_block(2 * m, 0), t_block(2 * m + 1, 0)
        send(a, a, xrec.at[0, m], xp, csem.at[4])
        send(b, b, xrec.at[2, m], xp, csem.at[4])
        send(b, b, xrec.at[1, m], xm, csem.at[4])
        send(a, a, xrec.at[2, m], xm, csem.at[4])

    def x_relay(m):
        b = 2 * m
        arrived(t_block(b, 3), xrec.at[0, m])
        send(t_block(b, 3), t_block(b, 3), xrec.at[2, m], xp, csem.at[4])
        b = 2 * m + 1
        arrived(t_block(b, 1), xrec.at[1, m])
        send(t_block(b, 1), t_block(b, 1), xrec.at[2, m], xm, csem.at[4])

    def x_rest(m):
        arrived(T.at[pl.ds(0, 128)], xrec.at[2, m])

    for m in range(2):
        l_t[m].wait()
        x_send(m)
    l_t[2].wait()

    @pl.when(core == 1)
    def _():
        pl.semaphore_wait(barrier, 10)
        pl.semaphore_signal(met, inc=1, device_id=sib, device_id_type=MESH)

    @pl.when(core == 0)
    def _():
        pl.semaphore_wait(met, 1)

    def rel(dz, dy):
        return (dz % NZ) * NY + dy % NY

    def piece(n, dz, dy):
        return W[n].at[(z + dz) % NZ, (y + dy) % NY]

    def fwd(n, dz, dy, peer, ddz, ddy):
        p = piece(n, dz, dy)
        send_weights(n, p, wrec.at[n // 2, rel(dz + ddz, dy + ddy)], peer)

    def to_sib(n, dz, dy):
        p = piece(n, dz, dy)
        send_weights(n, p, srec.at[n // 2, 1 if dz == 0 else 0], sib)

    def got(n, dz, dy):
        arrived(piece(n, dz, dy), wrec.at[n // 2, rel(dz, dy)])

    def all_from_sib(n):
        from_sib(n)
        arrived(W[n].at[pl.ds(0, 7)], srec.at[n // 2, 0])
        arrived(W[n].at[0, pl.ds(0, 3)], srec.at[n // 2, 1])

    def a_ysend(n):
        from_sib(n)
        fwd(n, 0, 0, yp, 0, -1)
        fwd(n, 0, 0, ym, 0, 1)
        fwd(n, 0, 0, y2, 0, 2)

    def a_zsend(n):
        fwd(n, 0, 0, zp, -1, 0)
        fwd(n, 0, 0, zm, 1, 0)

    def a_y(n):
        for dy in (1, 3, 2):
            got(n, 0, dy)
            fwd(n, 0, dy, zp, -1, 0)
            fwd(n, 0, dy, zm, 1, 0)
            to_sib(n, 0, dy)

    def a_hop(n, k, part=(0, 1, 2, 3)):
        for i in part:
            dy = (0, 1, 3, 2)[i]
            for dz in (-k, k) if k < 4 else (4,):
                got(n, dz, dy)
                if dz < 0 and (k < 3 or i % 2 == 0):
                    fwd(n, dz, dy, zp, -1, 0)
                if 0 < dz < 4 and (k < 3 or i % 2 == 1):
                    fwd(n, dz, dy, zm, 1, 0)
                to_sib(n, dz, dy)

    def ring(k):
        return (0,) if k == 0 else (-k, k) if k < 4 else (4,)

    def b_start(n):
        from_sib(n)
        fwd(n, 0, 0, zp, -1, 0)
        fwd(n, 0, 0, zm, 1, 0)

    def b_z(n, k):
        for dz in ring(k):
            got(n, dz, 0)
            if dz < 0:
                fwd(n, dz, 0, zp, -1, 0)
            elif k < 3:
                fwd(n, dz, 0, zm, 1, 0)
            to_sib(n, dz, 0)

    def b_zy(n, k):
        for dz in ring(k):
            fwd(n, dz, 0, yp, 0, -1)
            fwd(n, dz, 0, ym, 0, 1)

    def b_y(n, k):
        for dz in ring(k):
            up = k == 0 or 0 < dz < 4
            got(n, dz, 3)
            if up:
                fwd(n, dz, 3, yp, 0, -1)
            to_sib(n, dz, 3)
            got(n, dz, 1)
            if not up:
                fwd(n, dz, 1, ym, 0, 1)
            to_sib(n, dz, 1)

    def b_d(n, k):
        for dz in ring(k):
            got(n, dz, 2)
            to_sib(n, dz, 2)

    WO = (WOA, WOC)
    owner = z // 2
    place = (z + NZ - 2 * x) % NZ
    right = (place >= 1) & (place <= 4)
    dist = jnp.where(right, place - 1, (NZ - place) % NZ)
    u1 = jnp.where(right, 1, 0)
    u2 = 1 - u1
    onward = (at(z + jnp.where(right, 1, NZ - 1), y, core), x)
    back = (at(z + jnp.where(right, NZ - 1, 1), y, core), x)

    def wo_x():
        for h in range(2):
            here = (owner == x) & (core == h)

            @pl.when(here)
            def _(h=h):
                WO[h][z % 2, y, x, own_rows, :] = OWN[h]

            @pl.when(jnp.logical_not(here))
            def _(h=h):
                send(
                    OWN.at[h], WO[h].at[z % 2, y, x, own_rows], worec.at[(x + NX - owner) % NX],
                    (at(z, y, h), owner), csem.at[2 * h],
                )

    def wo_x_sent():
        for h in range(2):
            @pl.when(jnp.logical_not((owner == x) & (core == h)))
            def _(h=h):
                sent(OWN.at[h], csem.at[2 * h])

    def wo_share(h, u):
        unit = WO[h].at[u, y]
        send(unit, unit, woyrec.at[0, u], yp, wosend.at[0])
        send(unit, unit, woyrec.at[1, u], ym, wosend.at[0])
        send(unit, unit, wosib.at[0], sib, wosend.at[2])

    def wo_slot(h, k):
        if k < 4:
            @pl.when(dist == k)
            def _():
                unit = WO[h].at[u1, y]
                if k == 0:
                    arrived(WO[h].at[z % 2, y, x, sib_rows], worec.at[0])
                    for d in (1, 2, 3):
                        arrived(WO[h].at[z % 2, y, (x + d) % NX], worec.at[d])
                    send(unit, unit, wozrec.at[1], back, wozsem.at[1])
                else:
                    arrived(unit, wozrec.at[0])
                if k < 3:
                    send(unit, unit, wozrec.at[0], onward, wozsem.at[0])
                wo_share(h, u1)
        if k > 0:
            @pl.when(dist == k - 1)
            def _():
                unit = WO[h].at[u2, y]
                arrived(unit, wozrec.at[1])
                if k < 4:
                    send(unit, unit, wozrec.at[1], onward, wozsem.at[2])
                wo_share(h, u2)

    def wo_y(h):
        for u in range(2):
            for d, o in ((3, 0), (1, 1)):
                unit = WO[h].at[u, (y + d) % NY]
                arrived(unit, woyrec.at[o, u])
                if u == o:
                    send(unit, unit, woyrec.at[2, u], yp if u == 0 else ym, wosend.at[1])
                send(unit, unit, wosib.at[0], sib, wosend.at[2])

    def wo_d(h):
        for u in range(2):
            unit = WO[h].at[u, (y + 2) % NY]
            arrived(unit, woyrec.at[2, u])
            send(unit, unit, wosib.at[0], sib, wosend.at[2])

    def wo_end(h):
        arrived(WO[1 - h], wosib.at[0])

    def wo_sent():
        unit = WOA.at[0, 0]
        sent(WOA.at[0], wosend.at[0])
        sent(WOA.at[0, pl.ds(0, 2)], wosend.at[1])
        sent(WOA, wosend.at[2])

        @pl.when(dist < 3)
        def _():
            sent(unit, wozsem.at[0])

        @pl.when(dist < 4)
        def _():
            @pl.when(dist < 3)
            def _():
                sent(unit, wozsem.at[2])

        @pl.when(dist == 0)
        def _():
            sent(unit, wozsem.at[1])

    for cp in l_small:
        cp.wait()
    lane = lax.broadcasted_iota(jnp.int32, (GRID, HEAD), 1)
    line = lax.broadcasted_iota(jnp.int32, (GRID, HEAD), 0).astype(F32)
    by_row = lane < HEAD // 2
    negative = (lane // 32) % 2 == 0
    freq = freq_v[0:1, :]
    column_angle = line * freq
    column_cos, column_sin = jnp.cos(column_angle), jnp.sin(column_angle)
    first = (s * (ROWS // GRID)).astype(F32)
    row_angle = (lax.broadcasted_iota(jnp.int32, (16, HEAD), 0).astype(F32) + first) * freq
    row_cos, row_sin = jnp.cos(row_angle), jnp.sin(row_angle)
    for r in range(ROWS // GRID):
        COS[r * GRID : (r + 1) * GRID, :] = jnp.where(by_row, row_cos[r : r + 1, :], column_cos)
        sine = jnp.where(by_row, row_sin[r : r + 1, :], column_sin)
        SIN[r * GRID : (r + 1) * GRID, :] = jnp.where(negative, -sine, sine)

    negative = (lax.broadcasted_iota(jnp.int32, (256, HEAD), 1) // 32) % 2 == 0
    row256 = lax.broadcasted_iota(jnp.int32, (256, 1), 0)

    def rotate(u, cosine, sine):
        turned = jnp.where(negative, pltpu.roll(u, 96, 1), pltpu.roll(u, 32, 1))
        return (u * cosine + turned * sine).astype(BF16)

    def weight(ref, c0):
        return ref[:, :, :, c0 : c0 + 256].reshape(WIDTH, 256)

    def project(m):
        rows = slice(256 * m, 256 * m + 256)
        blocks = (2 * m, 2 * m + 1)
        cosine, sine = COS[rows, :], SIN[rows, :]
        q = jnp.dot(T[rows, :], weight(WA, 0), preferred_element_type=F32)
        for h in range(2):
            u = rotate(q[:, h * HEAD : (h + 1) * HEAD], cosine, sine)
            for i, b in enumerate(blocks):
                Q[b, h * 128 : (h + 1) * 128, :] = u[i * 128 : (i + 1) * 128]
        kv = jnp.dot(T[rows, :], weight(WA, 256), preferred_element_type=F32)
        k = rotate(kv[:, :HEAD], cosine, sine)
        v = kv[:, HEAD:].astype(BF16)
        for i, b in enumerate(blocks):
            KV[b + 1, :, 0:HEAD] = k[i * 128 : (i + 1) * 128]
            KV[b + 1, :, HEAD:] = v[i * 128 : (i + 1) * 128]

    def project_conv(m):
        rows = slice(256 * m, 256 * m + 256)
        blocks = (2 * m, 2 * m + 1)
        c_in = jnp.dot(T[rows, :], weight(WB, 0), preferred_element_type=F32)
        before = jnp.dot(T[rows, :], weight(WB, 256), preferred_element_type=F32)
        sec = (before * c_in).astype(BF16)
        for i, b in enumerate(blocks):
            SEC[b] = sec[i * 128 : (i + 1) * 128].astype(F32)
        if m == 0:
            ES[0] = sec[0:16]
        if m == 2:
            ES[1] = sec[240:256]
        after = jnp.dot(T[rows, :], weight(WD, 0), preferred_element_type=F32)
        for i, b in enumerate(blocks):
            GA[b] = after[i * 128 : (i + 1) * 128]

    row128 = lax.broadcasted_iota(jnp.int32, (128, 1), 0)
    taps = taps_v[...].astype(F32)

    def placed(b):
        p = PLACED.index(b)
        return slice(128 * p, 128 * p + 128)

    def convolve(b):
        sec = SEC[b]
        if b > 0:
            low = SEC[b - 1, 127:128, :]
        else:
            low = jnp.where(s > 0, ER[0].astype(F32)[15:16, :], 0.0)
        if b < 5:
            high = SEC[b + 1, 0:1, :]
        else:
            high = jnp.where(s < NSP - 1, ER[1].astype(F32)[0:1, :], 0.0)
        before = jnp.where(row128 == 0, low, pltpu.roll(sec, 1, 0))
        later = jnp.where(row128 == 127, high, pltpu.roll(sec, 127, 0))
        mix = before * taps[0:1] + sec * taps[1:2] + later * taps[2:3]
        MC[x, placed(b), :] = (GA[b] * mix).astype(BF16)

    qi = lax.broadcasted_iota(jnp.int32, (256, 384), 0) % 128
    kj = lax.broadcasted_iota(jnp.int32, (256, 384), 1)
    inside = (kj >= qi) & (kj <= qi + 256)
    sink_col = jnp.where(row256 < 128, sink[0], sink[1])

    def attend(b):
        keys = KV[b : b + 3, :, 0:HEAD].reshape(384, HEAD)
        values = KV[b : b + 3, :, HEAD:].reshape(384, HEAD)
        scores = nt_dot(Q[b], keys) * HEAD ** (-0.5)
        valid = inside
        if b == 0:
            valid = valid & ((kj >= 128) | (s > 0))
        if b == 5:
            valid = valid & ((kj < 256) | (s < NSP - 1))
        scores = jnp.where(valid, scores, NEG_BIG)
        top = jnp.maximum(jnp.max(scores, 1, keepdims=True), sink_col)
        w = jnp.exp(scores - top)
        total = jnp.sum(w, 1, keepdims=True) + jnp.exp(sink_col - top)
        probs = (w / total).astype(BF16)
        o = jnp.dot(probs, values, preferred_element_type=F32).astype(BF16)
        rows = placed(b)
        MA[x, rows, 0:HEAD] = o[:128]
        MA[x, rows, HEAD : 2 * HEAD] = o[128:]

    def halo_send(side):
        if side == 0:
            send(KV.at[1], KV.at[7], hrec.at[0], sm, csem.at[5])
        else:
            send(KV.at[6], KV.at[0], hrec.at[1], sp, csem.at[5])

    def edge_send(side):
        if side == 0:
            send(ES.at[0], ER.at[1], hrec.at[2], sm, csem.at[6])
        else:
            send(ES.at[1], ER.at[0], hrec.at[3], sp, csem.at[6])

    def halo_wait():
        arrived(KV.at[0], hrec.at[1])
        arrived(KV.at[7], hrec.at[0])

    def edge_wait():
        arrived(ER.at[0], hrec.at[3])
        arrived(ER.at[1], hrec.at[2])

    M = (MA, MC)

    def mix(h, d, r0, n):
        return M[h].at[(x + d) % NX, pl.ds(r0, n)]

    def mix_send(h, g):
        blk = mix(h, 0, 256 * g, 256)
        send(blk, blk, mixrec.at[2 * g + h, 0], xp, csem.at[7])
        send(blk, blk, mixrec.at[2 * g + h, 1], xm, csem.at[7])

    def mix_relay(h, g):
        arrived(mix(h, 3, 256 * g, 256), mixrec.at[2 * g + h, 0])
        blk = mix(h, 3, 256 * g, 128)
        send(blk, blk, mixrec.at[2 * g + h, 2], xp, csem.at[7])
        arrived(mix(h, 1, 256 * g, 256), mixrec.at[2 * g + h, 1])
        blk = mix(h, 1, 256 * g + 128, 128)
        send(blk, blk, mixrec.at[2 * g + h, 2], xm, csem.at[7])

    def partial(g, d):
        o = (x + d) % NX
        rows = slice(256 * g, 256 * g + 256)
        return sum(
            nt_dot(M[h][o, rows, :], WO[h][:, :, pl.ds(o, 1)].reshape(QUARTER, 256)) for h in range(2)
        )

    def final_near(g):
        PX[g] = partial(g, 0) + partial(g, 1) + partial(g, 3)

    def final_far(g):
        for h in range(2):
            arrived(mix(h, 2, 256 * g, 256), mixrec.at[2 * g + h, 2])
        PX[g] += partial(g, 2)
        for half in range(2):
            rows = slice(128 * half, 128 * half + 128)
            t = PX[g, rows, :]
            mean = jnp.sum(t, 1, keepdims=True) * (1.0 / QUARTER)
            m2 = jnp.sum(jnp.square(t - mean), 1, keepdims=True)
            lane = lax.broadcasted_iota(jnp.int32, (128, 128), 1)
            both = jnp.where(lane == 0, mean, m2)
            ST[g, 0, half] = jnp.transpose(both)[0:8, :]
        for d, peer, slot in ((1, xp, 3), (3, xm, 1), (2, x2, 2)):
            send(ST.at[g, 0], ST.at[g, slot], strec.at[g], peer, csem.at[9])

    def finish(g):
        arrived(ST.at[g, pl.ds(1, 3)], strec.at[g])
        for half in range(2):
            rows = slice(128 * half, 128 * half + 128)
            parts = [ST[g, slot, half] for slot in range(4)]
            means = [p[0:1, :] for p in parts]
            mean = (means[0] + means[1] + means[2] + means[3]) * 0.25
            m2 = sum(p[1:2, :] for p in parts)
            for m in means:
                m2 = m2 + QUARTER * jnp.square(m - mean)
            scale = lax.rsqrt(m2 * (1.0 / WIDTH) + EPS)
            line = lax.broadcasted_iota(jnp.int32, (128, 128), 0)
            columns = jnp.transpose(jnp.where(line == 0, mean, scale))
            normed = (PX[g, rows, :] - columns[:, 0:1]) * columns[:, 1:2] * gain_v[0:1, :]
            out[PLACED[2 * g + half] * 128 : PLACED[2 * g + half] * 128 + 128, :] = normed.astype(BF16)

    outs = []
    on_core(
        0,
        (a_ysend, 0), (a_zsend, 0), (a_y, 0), (a_hop, 0, 1),
        (x_relay, 0), (wo_x,), (x_relay, 1), (x_send, 2),
        (a_hop, 0, 2), (a_hop, 0, 3), (wo_slot, 0, 0), (a_hop, 0, 4),
    )
    on_core(
        1,
        (b_start, 1), (b_zy, 1, 0), (b_start, 3),
        (b_z, 1, 1), (b_zy, 1, 1), (b_zy, 3, 0), (b_z, 3, 1), (b_zy, 3, 1),
        (b_z, 1, 2), (b_zy, 1, 2), (b_y, 1, 0), (b_z, 3, 2), (b_zy, 3, 2), (b_y, 3, 0), (b_y, 1, 1),
        (x_relay, 0), (wo_x,), (x_relay, 1), (x_send, 2),
        (b_z, 1, 3), (b_zy, 1, 3), (b_y, 3, 1), (b_z, 3, 3), (b_zy, 3, 3),
        (b_d, 1, 0), (b_d, 3, 0), (b_y, 1, 2), (b_d, 1, 1), (b_y, 3, 2),
        (b_z, 1, 4), (b_zy, 1, 4), (b_d, 3, 1), (b_z, 3, 4), (b_zy, 3, 4),
        (b_y, 1, 3), (b_y, 3, 3), (b_d, 1, 2), (b_d, 3, 2), (b_y, 1, 4), (b_y, 3, 4),
        (b_d, 1, 3), (b_d, 3, 3), (wo_slot, 1, 0), (all_from_sib, 0),
    )
    x_rest(0)
    project(0)
    halo_send(0)
    on_core(0, (x_relay, 2), (wo_slot, 0, 1))
    on_core(1, (x_relay, 2), (b_d, 1, 4), (b_d, 3, 4), (wo_slot, 1, 1))
    x_rest(1)
    project(1)
    attend(1)
    attend(2)
    mix_send(0, 0)
    on_core(0, (all_from_sib, 1), (all_from_sib, 3))
    project_conv(0)
    edge_send(0)
    project_conv(1)
    convolve(1)
    convolve(2)
    mix_send(1, 0)
    on_core(0, (wo_slot, 0, 2))
    on_core(1, (wo_slot, 1, 2))
    x_rest(2)
    project(2)
    halo_send(1)
    attend(3)
    attend(4)
    mix_send(0, 1)
    mix_relay(0, 0)
    project_conv(2)
    edge_send(1)
    convolve(3)
    convolve(4)
    mix_send(1, 1)
    on_core(0, (wo_slot, 0, 3))
    on_core(1, (wo_slot, 1, 3))
    mix_relay(1, 0)
    halo_wait()
    attend(0)
    attend(5)
    mix_send(0, 2)
    edge_wait()
    convolve(0)
    convolve(5)
    mix_send(1, 2)
    on_core(0, (wo_slot, 0, 4))
    on_core(1, (wo_slot, 1, 4))
    mix_relay(0, 1)
    on_core(0, (wo_y, 0))
    on_core(1, (wo_y, 1))
    mix_relay(1, 1)
    on_core(0, (wo_d, 0), (wo_end, 0))
    on_core(1, (wo_d, 1), (wo_end, 1))
    mix_relay(0, 2)
    mix_relay(1, 2)
    wo_x_sent()
    wo_sent()
    assert set(counts.values()) == {62}
    for n, w in W.items():
        sent(w.at[z, y, own_rows], csem.at[ICS[n]])

        @pl.when(core == n % 2)
        def _(n=n, w=w):
            sent(w, wsem.at[n // 2, 0])
            sent(w.at[pl.ds(0, 7)], wsem.at[n // 2, 1])
            sent(w.at[0, pl.ds(0, 2)], wsem.at[n // 2, 2])
    sent(T.at[pl.ds(0, 576)], csem.at[4])
    sent(KV.at[pl.ds(0, 2)], csem.at[5])
    sent(ES, csem.at[6])
    final_near(0)
    final_far(0)
    final_near(1)
    final_far(1)
    final_near(2)
    final_far(2)
    finish(0)
    finish(1)
    finish(2)
    sent(T.at[pl.ds(0, 576)], csem.at[7])
    sent(ST.at[:, pl.ds(0, 3)], csem.at[9])


def body(
    tokens, query_weight, key_projection, value_projection, conv_in_weight, conv_gate_out,
    conv_gate_in, conv_taps, head_sink_logit, out_attn_weight, out_conv_weight, out_gain,
):
    half = HEAD // 2
    inverse = np.float32(THETA) ** (-np.arange(0, half, 2, dtype=np.float32) / np.float32(half))
    freq = jnp.asarray(np.tile(inverse.astype(np.float32), 4)[None, :])
    anywhere = pl.BlockSpec(memory_space=pl.ANY)
    specs = [anywhere] * 13
    dma = pltpu.SemaphoreType.DMA
    call = pl.pallas_call(
        kernel,
        out_shape=jax.ShapeDtypeStruct((ROWS, QUARTER), BF16),
        in_specs=specs,
        out_specs=pl.BlockSpec(memory_space=pltpu.VMEM),
        scratch_shapes=[
            pltpu.VMEM((ROWS, WIDTH), BF16),
            pltpu.VMEM((NZ, NY, 64, 512), BF16),
            pltpu.VMEM((NZ, NY, 64, 512), BF16),
            pltpu.VMEM((NZ, NY, 64, 256), BF16),
            pltpu.VMEM((2, NY, NX, 64, 256), BF16),
            pltpu.VMEM((2, NY, NX, 64, 256), BF16),
            pltpu.VMEM((2, 32, 256), BF16),
            pltpu.VMEM((8, 128, 256), BF16),
            pltpu.VMEM((6, 256, 128), BF16),
            pltpu.VMEM((6, 128, 256), F32),
            pltpu.VMEM((6, 128, 256), F32),
            pltpu.VMEM((NX, ROWS, 256), BF16),
            pltpu.VMEM((NX, ROWS, 256), BF16),
            pltpu.VMEM((2, 16, 256), BF16),
            pltpu.VMEM((2, 16, 256), BF16),
            pltpu.VMEM((ROWS, HEAD), F32),
            pltpu.VMEM((ROWS, HEAD), F32),
            pltpu.VMEM((3, 256, QUARTER), F32),
            pltpu.VMEM((3, 4, 2, 8, 128), F32),
            pltpu.VMEM((3, 256), BF16),
            pltpu.VMEM((1, QUARTER), F32),
            pltpu.VMEM((1, HEAD), F32),
            pltpu.SMEM((2,), F32),
            dma((16,)),
            pltpu.SemaphoreType.REGULAR,
            dma((10,)),
            dma((2, 3)),
            dma((2, 32)),
            dma((2, 2)),
            dma((4,)),
            dma((3, 3)),
            dma((4,)),
            dma((6, 3)),
            dma((3,)),
            dma((1,)),
            dma((4,)),
            dma((2,)),
            dma((3,)),
            dma((3, 2)),
            dma((3,)),
            dma((1,)),
        ],
        compiler_params=pltpu.CompilerParams(
            collective_id=0, has_side_effects=True, vmem_limit_bytes=40 * 1024 * 1024
        ),
    )
    operands = [
        tokens, query_weight, key_projection, value_projection, conv_in_weight, conv_gate_out,
        conv_gate_in, conv_taps, head_sink_logit, out_attn_weight.T, out_conv_weight.T,
        out_gain.reshape(1, -1), freq,
    ]
    return call(*[
        pltpu.with_memory_space_constraint(a, pltpu.HBM) for a in operands
    ])


def solution(mesh):
    return jax.shard_map(
        body,
        mesh=mesh,
        in_specs=(
            P("sp", "tp"),
            P("sp", "tp"),
            P("sp", "tp"),
            P("sp", "tp"),
            P("sp", "tp"),
            P("sp", "tp"),
            P("sp", "tp"),
            P(None, "tp"),
            P("tp"),
            P("tp", "sp"),
            P("tp", "sp"),
            P("tp"),
        ),
        out_specs=P("sp", "tp"),
        check_vma=False,
    )
```
